256 devices in a mesh: ep: 128 (over z, y, x), tp: 2 (over core).
Axes of the slice: x: 4, y: 4, z: 8, core: 2. Of those that a mesh axis runs over, the one named last changes fastest.
Arguments:
- tokens: bfloat16 [512, 2048], P('ep'), may hold values from -6 to 6
- lengths: int32 [512], P('ep'), may hold values from 1 to 1024
- cache_keys: bfloat16 [512, 1024, 512], P('ep', None, 'tp'), may hold values from -640 to 640
- cache_values: bfloat16 [512, 1024, 512], P('ep', None, 'tp'), may hold values from -6 to 6
- norm0_gain: float32 [2048], replicated, may hold values from 0.1 to 1.9
- query_weight: bfloat16 [2048, 1536], P('ep', 'tp'), may hold values from -0.125 to 0.125
- key_weight: bfloat16 [2048, 512], P('ep', 'tp'), may hold values from -0.21875 to 0.21875
- value_weight: bfloat16 [2048, 512], P('ep', 'tp'), may hold values from -0.125 to 0.125
- mix_lambda: float32 [6], P('tp'), may hold values from 0.3 to 0.8
- head_gain: float32 [256], replicated, may hold values from 0.1 to 1.9
- out_weight: bfloat16 [1536, 2048], P('tp', 'ep'), may hold values from -0.15625 to 0.15625
- norm1_gain: float32 [2048], replicated, may hold values from 0.1 to 1.9
- group_ids: int32 [512], P('ep'), may hold values from 0 to 31, as said below
- member_ids: int32 [512, 2], P('ep'), may hold values from 0 to 3, as said below
- group_weight: float32 [512], P('ep'), may hold values from 0.3 to 1
- member_weights: float32 [512, 2], P('ep'), may hold values from 0.2 to 1
- expert_gate: bfloat16 [128, 2048, 512], P('ep', None, 'tp'), may hold values from -0.125 to 0.125
- expert_up: bfloat16 [128, 2048, 512], P('ep', None, 'tp'), may hold values from -0.125 to 0.125
- expert_down: bfloat16 [128, 512, 2048], P('ep', 'tp'), may hold values from -0.25 to 0.25
- norm2_gain: float32 [2048], P('tp'), may hold values from 0.1 to 1.9
Outputs:
- result: bfloat16 [512, 2048], P('ep', 'tp')
The draws below stay inside these ranges and needn't reach their ends.
Inputs may be any that keep to these rules, and one draw needn't show every extreme that they name: `group_ids`: every group is named by exactly 16 tokens; the 4 tokens of one device name different groups. `member_ids`: A token's 2 members are different; no expert is used by more than 16 tokens, and some expert by exactly 16.
All inputs are finite; a program needn't handle non-finite values.
Results may differ from the reference program's by a relative error of at most 0.015.
Values may be sent and summed in bfloat16 or wider, within the bound.
No kernel may reach another device: no remote copies, remote signals or barrier semaphores. Data moves between devices by JAX's collectives and lax.ppermute only.
A program may use at most 64 MiB of HBM per device.

```python
import jax
import jax.numpy as jnp
from jax import lax

D = 2048
HEADS = 6
KV_HEADS = 2
HD = 128
VH = 256
FF = 512
EPG = 4
TOPK = 2
CACHE = 1024
SEQ_DEV = 4
SEQS = 512
EXPERTS = 128
GROUPS = 32
ROWS_GROUP = 16


def routing_draw(key):
    devices = SEQS // SEQ_DEV
    base = jax.random.permutation(jax.random.fold_in(key, 11), devices).astype(jnp.int32)
    offsets = jax.random.permutation(jax.random.fold_in(key, 16), GROUPS)[:SEQ_DEV].astype(jnp.int32)
    groups = ((base[:, None] + offsets[None, :]) % GROUPS).reshape(SEQS).astype(jnp.int32)
    leader = jax.random.randint(jax.random.fold_in(key, 12), (GROUPS,), 0, EPG)
    flags = jax.random.randint(jax.random.fold_in(key, 13), (GROUPS,), 0, 2)
    forced = jax.random.randint(jax.random.fold_in(key, 14), (), 0, GROUPS)
    flags = flags.at[forced].set(1)
    scores = jax.random.randint(jax.random.fold_in(key, 15), (SEQS, EPG), 0, 2 ** 20) * EPG
    scores = scores + jnp.arange(EPG, dtype=jnp.int32)[None, :]
    boost = (jnp.arange(EPG, dtype=jnp.int32)[None, :] == leader[groups][:, None]) & (flags[groups][:, None] == 1)
    scores = scores + boost.astype(jnp.int32) * 2 ** 26
    members = lax.top_k(scores, TOPK)[1]
    return (groups, members.astype(jnp.int32))


def draw_group_ids(key, part):
    return routing_draw(key)[0]


def draw_member_ids(key, part):
    return routing_draw(key)[1]


def draw_lengths(key, part):
    filled = jax.random.randint(jax.random.fold_in(key, 21), (SEQS,), 1, CACHE + 1)
    longest = jax.random.randint(jax.random.fold_in(key, 22), (), 0, SEQS)
    return filled.at[longest].set(CACHE).astype(jnp.int32)


def draw_cache_keys(key, part):
    base = jnp.clip(jax.random.normal(jax.random.fold_in(key, 31), (SEQS, CACHE, KV_HEADS * 2 * HD), jnp.float32), -6.0, 6.0) * 1.75
    return base.astype(jnp.bfloat16)


def block_scale(rng, dims, pieces, smallest, largest):
    def one(dim, blocks):
        steps = jax.random.uniform(jax.random.fold_in(jax.random.fold_in(rng, 6), dim), (blocks,), jnp.float32, smallest / len(pieces), largest / len(pieces))
        return jnp.repeat(jnp.exp(steps), dims[dim] // blocks).reshape((-1,) + (1,) * (len(dims) - dim - 1))

    level = one(*pieces[0])
    for cut in pieces[1:]:
        level = level * one(*cut)
    return level


def scatter_about(own_key, extent, scale, bound, cuts=(), kind=jnp.bfloat16):
    values = jax.random.normal(own_key, extent, jnp.float32) * scale
    if len(cuts) > 0:
        values = block_scale(own_key, extent, cuts, -0.22, 0.18) * values
    return jnp.clip(values, min=-bound, max=bound).astype(kind)


def setup_inputs(seed: int = 0) -> dict:
    key_of = jax.random.split(jax.random.key(seed), 21)
    tokens = scatter_about(key_of[0], (SEQS, D), 1.0, 6.0, ((0, 128),))
    lengths = draw_lengths(jax.random.fold_in(key_of[20], 71), 0)
    cache_keys = draw_cache_keys(jax.random.fold_in(key_of[20], 71), 0)
    cache_values = scatter_about(key_of[3], (SEQS, CACHE, KV_HEADS * VH), 1.0, 6.0, ((0, 128), (2, 2)))
    norm0_gain = jnp.clip(1.0 + 0.18 * jax.random.normal(key_of[4], (D,), jnp.float32), 0.1, 1.9)
    query_weight = scatter_about(key_of[5], (D, HEADS * 2 * HD), D ** -0.5, 0.125, ((0, 128), (1, 2)))
    key_weight = scatter_about(key_of[6], (D, KV_HEADS * 2 * HD), (D // 3) ** -0.5, 0.21875, ((0, 128), (1, 2)))
    value_weight = scatter_about(key_of[7], (D, KV_HEADS * VH), D ** -0.5, 0.125, ((0, 128), (1, 2)))
    mix_lambda = jnp.clip(0.3 + 0.5 * jax.random.uniform(key_of[8], (HEADS,), jnp.float32) ** block_scale(key_of[8], (HEADS,), ((0, 2),), -0.2, 0.2), 0.3, 0.8)
    head_gain = jnp.clip(1.0 + 0.18 * jax.random.normal(key_of[9], (VH,), jnp.float32), 0.1, 1.9)
    out_weight = scatter_about(key_of[10], (HEADS * VH, D), (HEADS * VH) ** -0.5, 0.15625, ((0, 2), (1, 128)))
    norm1_gain = jnp.clip(1.0 + 0.18 * jax.random.normal(key_of[11], (D,), jnp.float32), 0.1, 1.9)
    group_ids = draw_group_ids(jax.random.fold_in(key_of[20], 71), 0)
    member_ids = draw_member_ids(jax.random.fold_in(key_of[20], 71), 0)
    group_weight = jnp.clip(0.3 + 0.7 * jax.random.uniform(key_of[14], (SEQS,), jnp.float32) ** block_scale(key_of[14], (SEQS,), ((0, 128),), -0.2, 0.2), 0.3, 1.0)
    member_weights = jnp.clip(0.2 + 0.8 * jax.random.uniform(key_of[15], (SEQS, TOPK), jnp.float32) ** block_scale(key_of[15], (SEQS, TOPK), ((0, 128),), -0.2, 0.2), 0.2, 1.0)
    expert_gate = scatter_about(key_of[16], (EXPERTS, D, FF), D ** -0.5, 0.125, ((0, 128), (2, 2)))
    expert_up = scatter_about(key_of[17], (EXPERTS, D, FF), D ** -0.5, 0.125, ((0, 128), (2, 2)))
    expert_down = scatter_about(key_of[18], (EXPERTS, FF, D), FF ** -0.5, 0.25, ((0, 128), (1, 2)))
    norm2_gain = jnp.clip(1.0 + 0.18 * jax.random.normal(key_of[19], (D,), jnp.float32), 0.1, 1.9)
    return dict(tokens=tokens, lengths=lengths, cache_keys=cache_keys, cache_values=cache_values, norm0_gain=norm0_gain, query_weight=query_weight, key_weight=key_weight, value_weight=value_weight, mix_lambda=mix_lambda, head_gain=head_gain, out_weight=out_weight, norm1_gain=norm1_gain, group_ids=group_ids, member_ids=member_ids, group_weight=group_weight, member_weights=member_weights, expert_gate=expert_gate, expert_up=expert_up, expert_down=expert_down, norm2_gain=norm2_gain)


ALPHA = 2.0 ** 0.25
EPS = 1e-05

def layer_norm(values, gain):
    mean = lax.optimization_barrier(jnp.mean(values, -1, keepdims=True))
    spread = lax.optimization_barrier(jnp.mean(jnp.square(values - mean), -1, keepdims=True))
    return (values - mean) * lax.rsqrt(spread + EPS) * gain

def attend_block(queries, new_keys, new_values, cache_keys, cache_values, lengths, mix_lambda, head_gain):
    seqs = queries.shape[0]
    span = cache_keys.shape[1]
    group = HEADS // KV_HEADS
    query_grid = queries.astype(jnp.float32).reshape(seqs, KV_HEADS, group, 2, HD)
    cached_keys = cache_keys.astype(jnp.float32).reshape(seqs, span, KV_HEADS, 2, HD)
    fresh_keys = new_keys.astype(jnp.float32).reshape(seqs, KV_HEADS, 2, HD)
    cached_values = cache_values.astype(jnp.float32).reshape(seqs, span, KV_HEADS, VH)
    fresh_values = new_values.astype(jnp.float32).reshape(seqs, KV_HEADS, VH)
    valid = (jnp.arange(span, dtype=jnp.int32)[None, :] < lengths[:, None])[:, None, None, :]
    scale = HD ** (-0.5)
    maps = []
    for which in range(2):
        cached = jnp.einsum('sghd,scgd->sghc', query_grid[:, :, :, which], cached_keys[:, :, :, which]) * scale
        fresh = jnp.einsum('sghd,sgd->sgh', query_grid[:, :, :, which], fresh_keys[:, :, which]) * scale
        highest = jnp.maximum(lax.optimization_barrier(jnp.max(jnp.where(valid, cached, -1e+30), -1)), fresh)
        spread = jnp.where(valid, jnp.exp(cached - highest[..., None]), 0.0)
        itself = jnp.exp(fresh - highest)
        total = lax.optimization_barrier(jnp.sum(spread, -1)) + itself
        maps.append((spread / total[..., None], itself / total))
    lambdas = mix_lambda.reshape(1, KV_HEADS, group)
    cached_weight = (maps[0][0] - lambdas[..., None] * maps[1][0]).astype(jnp.bfloat16)
    fresh_weight = (maps[0][1] - lambdas * maps[1][1]).astype(jnp.bfloat16)
    head_out = jnp.einsum('sghc,scgv->sghv', cached_weight.astype(jnp.float32), cached_values)
    head_out = head_out + fresh_weight.astype(jnp.float32)[..., None] * fresh_values[:, :, None, :]
    head_out = head_out * lax.rsqrt(lax.optimization_barrier(jnp.mean(head_out * head_out, -1, keepdims=True)) + EPS) * head_gain
    return head_out.astype(jnp.bfloat16).reshape(seqs, HEADS * VH)

def reference(tokens, lengths, cache_keys, cache_values, norm0_gain, query_weight, key_weight, value_weight, mix_lambda, head_gain, out_weight, norm1_gain, group_ids, member_ids, group_weight, member_weights, expert_gate, expert_up, expert_down, norm2_gain):
    normed = layer_norm(tokens.astype(jnp.float32), norm0_gain).astype(jnp.bfloat16)
    queries = jnp.dot(normed, query_weight, preferred_element_type=jnp.float32).astype(jnp.bfloat16)
    new_keys = jnp.dot(normed, key_weight, preferred_element_type=jnp.float32).astype(jnp.bfloat16)
    new_values = jnp.dot(normed, value_weight, preferred_element_type=jnp.float32).astype(jnp.bfloat16)
    blocks = SEQS // SEQ_DEV

    def shape_blocks(array):
        return array.reshape((blocks, SEQ_DEV) + array.shape[1:])

    def one_block(items):
        return attend_block(items[0], items[1], items[2], items[3], items[4], items[5], mix_lambda, head_gain)
    attended = lax.map(one_block, (shape_blocks(queries), shape_blocks(new_keys), shape_blocks(new_values), shape_blocks(cache_keys), shape_blocks(cache_values), shape_blocks(lengths)))
    attended = attended.reshape(SEQS, HEADS * VH)
    mix = jnp.dot(attended, out_weight, preferred_element_type=jnp.float32).astype(jnp.bfloat16)
    stream = (ALPHA * normed.astype(jnp.float32) + mix.astype(jnp.float32)).astype(jnp.bfloat16)
    settled = layer_norm(stream.astype(jnp.float32), norm1_gain).astype(jnp.bfloat16)
    expert_ids = (group_ids[:, None] * EPG + member_ids).astype(jnp.int32)
    share = group_weight[:, None] * member_weights
    slots = jnp.arange(ROWS_GROUP, dtype=jnp.int32)

    def expert_step(total, expert):
        hits = expert_ids == expert
        named = jnp.any(hits, 1)
        coefficient = lax.optimization_barrier(jnp.sum(jnp.where(hits, share, 0.0), 1))
        picked = jnp.nonzero(named, size=ROWS_GROUP, fill_value=0)[0].astype(jnp.int32)
        valid = slots < jnp.sum(named.astype(jnp.int32))
        chosen = jnp.where(valid, coefficient[picked], 0.0)
        rows = settled[picked]
        gate = jnp.dot(rows, expert_gate[expert], preferred_element_type=jnp.float32)
        upward = jnp.dot(rows, expert_up[expert], preferred_element_type=jnp.float32)
        hidden = (jax.nn.silu(gate) * upward).astype(jnp.bfloat16)
        output = jnp.dot(hidden, expert_down[expert], preferred_element_type=jnp.float32) * chosen[:, None]
        return (total.at[picked].add(output), None)
    routed, _ = lax.scan(expert_step, jnp.zeros((SEQS, D), jnp.float32), jnp.arange(EXPERTS, dtype=jnp.int32))
    mixed = ALPHA * settled.astype(jnp.float32) + routed
    return layer_norm(mixed, norm2_gain).astype(jnp.bfloat16)
```

```python
import jax
import jax.numpy as jnp
from jax import lax
from jax.sharding import Mesh
from jax.sharding import PartitionSpec as P

EPG = 4
EP = ("z", "y", "x")
ROW = ("y", "x")

ALPHA = 2.0**0.25
EPS = 1e-05


def swap(array, axis):
    return lax.all_to_all(array, axis, 0, 0, tiled=True)


def to_all(array, axis):
    return swap(jnp.broadcast_to(array[None], (lax.axis_size(axis), *array.shape)), axis)


def layer_norm(values, gain):
    mean = jnp.mean(values, -1, keepdims=True)
    spread = jnp.mean(jnp.square(values - mean), -1, keepdims=True)
    return (values - mean) * lax.rsqrt(spread + EPS) * gain


def attend(queries, new_keys, new_values, cache_keys, cache_values, lengths, mix_lambda, head_gain):
    seqs = queries.shape[0]
    span = cache_keys.shape[1]
    vwidth = head_gain.shape[0]
    kv_local = cache_values.shape[2] // vwidth
    hwidth = cache_keys.shape[2] // (2 * kv_local)
    heads_local = mix_lambda.shape[0]
    group = heads_local // kv_local
    query_grid = queries.reshape(seqs, kv_local, group, 2, hwidth)
    cached_keys = cache_keys.reshape(seqs, span, kv_local, 2, hwidth)
    fresh_keys = new_keys.reshape(seqs, kv_local, 2, hwidth)
    cached_values = cache_values.reshape(seqs, span, kv_local, vwidth)
    fresh_values = new_values.reshape(seqs, kv_local, vwidth)
    valid = (jnp.arange(span, dtype=jnp.int32)[None, :] < lengths[:, None])[:, None, None, :]
    scale = hwidth ** (-0.5)
    maps = []
    for which in range(2):
        cached = (
            jnp.einsum(
                "sghd,scgd->sghc",
                query_grid[:, :, :, which],
                cached_keys[:, :, :, which],
                preferred_element_type=jnp.float32,
            )
            * scale
        )
        fresh = (
            jnp.einsum(
                "sghd,sgd->sgh",
                query_grid[:, :, :, which],
                fresh_keys[:, :, which],
                preferred_element_type=jnp.float32,
            )
            * scale
        )
        highest = jnp.maximum(jnp.max(jnp.where(valid, cached, -1e30), -1), fresh)
        spread = jnp.where(valid, jnp.exp(cached - highest[..., None]), 0.0)
        itself = jnp.exp(fresh - highest)
        total = jnp.sum(spread, -1) + itself
        maps.append((spread / total[..., None], itself / total))
    lambdas = mix_lambda.reshape(1, kv_local, group)
    cached_weight = (maps[0][0] - lambdas[..., None] * maps[1][0]).astype(jnp.bfloat16)
    fresh_weight = (maps[0][1] - lambdas * maps[1][1]).astype(jnp.bfloat16)
    head_out = jnp.einsum(
        "sghc,scgv->sghv", cached_weight, cached_values, preferred_element_type=jnp.float32
    )
    head_out = (
        head_out
        + fresh_weight.astype(jnp.float32)[..., None]
        * fresh_values.astype(jnp.float32)[:, :, None, :]
    )
    head_out = (
        head_out * lax.rsqrt(jnp.mean(head_out * head_out, -1, keepdims=True) + EPS) * head_gain
    )
    return head_out.astype(jnp.bfloat16).reshape(seqs, heads_local * vwidth)


def shards(
    tokens,
    lengths,
    cache_keys,
    cache_values,
    norm0_gain,
    query_weight,
    key_weight,
    value_weight,
    mix_lambda,
    head_gain,
    out_weight,
    norm1_gain,
    group_ids,
    member_ids,
    group_weight,
    member_weights,
    expert_gate,
    expert_up,
    expert_down,
    norm2_gain,
):
    seqs, width = tokens.shape
    deep = lax.axis_size("z")
    experts = lax.axis_size(EP)
    halves = lax.axis_size("tp")
    half = width // halves
    block = width // deep
    query_cols = query_weight.shape[1]
    key_cols = key_weight.shape[1]
    value_cols = value_weight.shape[1]
    proj_cols = query_cols + key_cols + value_cols
    expert_ids = group_ids[:, None] * EPG + member_ids
    share = group_weight[:, None] * member_weights

    own_weights = jnp.concatenate((query_weight, key_weight, value_weight, out_weight.T), 1)
    weights = to_all(own_weights, ROW).reshape(block, -1)
    weight_in = weights[:, :proj_cols]
    weight_out = weights[:, proj_cols:]

    normed = layer_norm(tokens.astype(jnp.float32), norm0_gain).astype(jnp.bfloat16)
    columns = swap(normed.reshape(seqs, deep, block).transpose(1, 0, 2), "z")
    partial = jnp.dot(
        columns.reshape(deep * seqs, block), weight_in, preferred_element_type=jnp.float32
    )
    projected = jnp.sum(swap(partial.reshape(deep, seqs, proj_cols), "z"), 0).astype(jnp.bfloat16)
    queries = projected[:, :query_cols]
    new_keys = projected[:, query_cols : query_cols + key_cols]
    new_values = projected[:, query_cols + key_cols :]
    attended = attend(
        queries, new_keys, new_values, cache_keys, cache_values, lengths, mix_lambda, head_gain
    )
    everyone = to_all(attended, "z").reshape(deep * seqs, -1)
    partial_mix = lax.dot_general(
        everyone, weight_out, (((1,), (1,)), ((), ())), preferred_element_type=jnp.float32
    ).astype(jnp.bfloat16)
    doubled = jnp.broadcast_to(
        partial_mix.reshape(deep, 1, seqs, block), (deep, halves, seqs, block)
    )
    back = swap(doubled.reshape(deep * halves, seqs, block), ("z", "tp"))
    mix = jnp.sum(back.astype(jnp.float32).reshape(deep, halves, seqs, block), 1)
    mix = mix.transpose(1, 0, 2).reshape(seqs, width).astype(jnp.bfloat16)
    stream = (ALPHA * normed.astype(jnp.float32) + mix.astype(jnp.float32)).astype(jnp.bfloat16)
    settled = layer_norm(stream.astype(jnp.float32), norm1_gain).astype(jnp.bfloat16)

    targets = lax.iota(jnp.int32, experts)
    select = jnp.any(expert_ids[None, :, :] == targets[:, None, None], 2)
    tiles = settled.reshape(1, seqs, width // 128, 128)
    sending = jnp.sum(
        jnp.where(select[:, :, None, None], tiles, jnp.zeros_like(tiles)).astype(jnp.float32), 1
    ).astype(jnp.bfloat16)
    rows = swap(sending, EP).reshape(experts, width)
    gate = jnp.dot(rows, expert_gate[0], preferred_element_type=jnp.float32)
    upward = jnp.dot(rows, expert_up[0], preferred_element_type=jnp.float32)
    hidden = (jax.nn.silu(gate) * upward).astype(jnp.bfloat16)
    output = jnp.dot(hidden, expert_down[0], preferred_element_type=jnp.float32)
    output = output.astype(jnp.bfloat16).reshape(experts * halves, half // 128, 128)
    returned = swap(output, EP + ("tp",)).reshape(experts, halves, half // 128, 128)
    both = jnp.sum(returned.astype(jnp.float32), 1)
    combine = jnp.sum(
        jnp.where(expert_ids[:, :, None] == targets[None, None, :], share[:, :, None], 0.0), 1
    )
    routed = jnp.sum(combine[:, :, None, None] * both[None], 1).reshape(seqs, half)
    own = lax.dynamic_slice_in_dim(settled, lax.axis_index("tp") * half, half, 1)
    mixed = ALPHA * own.astype(jnp.float32) + routed
    sums = lax.psum(jnp.stack((jnp.sum(mixed, 1), jnp.sum(mixed * mixed, 1))), "tp")
    mean = sums[0] / width
    spread = sums[1] / width - mean * mean
    result = (mixed - mean[:, None]) * lax.rsqrt(spread[:, None] + EPS) * norm2_gain
    return result.astype(jnp.bfloat16)


def solution(mesh):
    torus = Mesh(mesh.devices.reshape(8, 4, 4, mesh.shape["tp"]), ("z", "y", "x", "tp"))
    return jax.shard_map(
        shards,
        mesh=torus,
        in_specs=(
            P(EP, None),
            P(EP),
            P(EP, None, "tp"),
            P(EP, None, "tp"),
            P(),
            P(EP, "tp"),
            P(EP, "tp"),
            P(EP, "tp"),
            P("tp"),
            P(),
            P("tp", EP),
            P(),
            P(EP),
            P(EP, None),
            P(EP),
            P(EP, None),
            P(EP, None, "tp"),
            P(EP, None, "tp"),
            P(EP, "tp", None),
            P("tp"),
        ),
        out_specs=P(EP, "tp"),
        check_vma=False,
    )
```

```python
import jax
import jax.numpy as jnp
from jax import lax
from jax.experimental import pallas as pl
from jax.experimental.pallas import tpu as pltpu
from jax.sharding import Mesh
from jax.sharding import PartitionSpec as P


EPG = 4
EP = ("z", "y", "x")
ROW = ("y", "x")

ALPHA = 2.0**0.25
EPS = 1e-05


def swap(array, axis):
    return lax.all_to_all(array, axis, 0, 0, tiled=True)


def to_all(array, axis):
    return swap(jnp.broadcast_to(array[None], (lax.axis_size(axis), *array.shape)), axis)


def layer_norm(values, gain):
    mean = jnp.mean(values, -1, keepdims=True)
    spread = jnp.mean(jnp.square(values - mean), -1, keepdims=True)
    return (values - mean) * lax.rsqrt(spread + EPS) * gain


def expert_kernel(side_ref, rows_ref, gain_ref, gate_ref, up_ref, down_ref, kept_ref, given_ref, settled_ref):
    halves, sources, deep, part = rows_ref.shape
    line = sources // deep
    slots = line * deep
    width = gate_ref.shape[0]
    half = width // halves

    def piece(c, t):
        block = rows_ref[t, c * line : (c + 1) * line].astype(jnp.float32)
        return block.reshape(slots, part)

    total = jnp.zeros((slots, part), jnp.float32)
    for c in range(deep):
        for t in range(halves):
            total = total + piece(c, t)
    mean = jnp.sum(total, 1, keepdims=True) * (1.0 / width)
    square = jnp.zeros((slots, part), jnp.float32)
    for c in range(deep):
        for t in range(halves):
            off = piece(c, t) - mean
            square = square + off * off
    scale = lax.rsqrt(jnp.sum(square, 1, keepdims=True) * (1.0 / width) + EPS)
    for c in range(deep):
        for t in range(halves):
            at = (c * halves + t) * part
            value = (piece(c, t) - mean) * scale * gain_ref[:, at : at + part]
            settled_ref[:, at : at + part] = value.astype(jnp.bfloat16)
    settled = settled_ref[...]
    gate = jnp.dot(settled, gate_ref[...], preferred_element_type=jnp.float32)
    upward = jnp.dot(settled, up_ref[...], preferred_element_type=jnp.float32)
    hidden = (gate * jax.nn.sigmoid(gate) * upward).astype(jnp.bfloat16)
    side = side_ref[0]

    def spread(output, out_ref):
        tiles = jnp.stack([output[:, j * 128 : (j + 1) * 128] for j in range(half // 128)], 0)
        tiles = jnp.transpose(tiles, (1, 0, 2)).astype(out_ref.dtype)
        for p in range(line):
            for s in range(deep):
                out_ref[s * line + p] = tiles[p * deep + s]

    given = down_ref[:, pl.ds(pl.multiple_of((1 - side) * half, half), half)]
    spread(jnp.dot(hidden, given, preferred_element_type=jnp.float32), given_ref)
    kept = down_ref[:, pl.ds(pl.multiple_of(side * half, half), half)]
    spread(jnp.dot(hidden, kept, preferred_element_type=jnp.float32), kept_ref)


def run_experts(side, rows, gain, gate, up, down):
    halves, sources, _, _ = rows.shape
    width = gate.shape[0]
    vm = pl.BlockSpec(memory_space=pltpu.VMEM)
    shape = (sources, width // halves // 128, 128)
    return pl.pallas_call(
        expert_kernel,
        out_shape=(jax.ShapeDtypeStruct(shape, jnp.float32), jax.ShapeDtypeStruct(shape, jnp.bfloat16)),
        in_specs=[pl.BlockSpec(memory_space=pltpu.SMEM)] + [vm] * 5,
        out_specs=(vm, vm),
        scratch_shapes=[pltpu.VMEM((sources, width), jnp.bfloat16)],
        name="experts",
    )(side.reshape(1), rows, gain.reshape(1, -1), gate, up, down)


def attend_kernel(lengths_ref, lambda_ref, parts_ref, keys_ref, values_ref, gain_ref, out_ref):
    deep, seqs, _ = parts_ref.shape
    _, width = keys_ref.shape[1:]
    hwidth = width // 2
    heads = lambda_ref.shape[0]
    pad = 4
    rows = 2 * pad
    f32 = jnp.float32
    total = parts_ref[0]
    for d in range(1, deep):
        total = total + parts_ref[d]
    total = total.astype(jnp.bfloat16).astype(f32)
    first = lax.broadcasted_iota(jnp.int32, (1, width), 1) < hwidth
    blank = jnp.zeros((1, width), f32)
    at = heads * width
    scores, fresh = [], []
    for s in range(seqs):
        query = [total[s : s + 1, h * width : (h + 1) * width] for h in range(heads)]
        ones = [jnp.where(first, q, 0.0) for q in query] + [blank] * (pad - heads)
        twos = [jnp.where(first, 0.0, q) for q in query] + [blank] * (pad - heads)
        grid = jnp.concatenate(ones + twos, 0)
        new_key = total[s : s + 1, at : at + width]
        fresh.append(jnp.sum(grid * new_key, 1, keepdims=True))
        scores.append(
            lax.dot_general(
                grid.astype(jnp.bfloat16),
                keys_ref[s],
                (((1,), (1,)), ((), ())),
                preferred_element_type=f32,
            )
        )
    scale = hwidth**-0.5
    cached = jnp.concatenate(scores, 0) * scale
    newest = jnp.concatenate(fresh, 0) * scale
    row = lax.broadcasted_iota(jnp.int32, (seqs * rows, 1), 0)
    filled = jnp.zeros((seqs * rows, 1), jnp.int32)
    lam = jnp.zeros((pad, 1), f32)
    for s in range(seqs):
        filled = jnp.where(row // rows == s, lengths_ref[s], filled)
    side_row = lax.broadcasted_iota(jnp.int32, (pad, 1), 0)
    for h in range(heads):
        lam = jnp.where(side_row == h, lambda_ref[h], lam)
    valid = lax.broadcasted_iota(jnp.int32, cached.shape, 1) < filled
    highest = jnp.maximum(jnp.max(jnp.where(valid, cached, -1e30), 1, keepdims=True), newest)
    spread = jnp.where(valid, jnp.exp(cached - highest), 0.0)
    itself = jnp.exp(newest - highest)
    inverse = 1.0 / (jnp.sum(spread, 1, keepdims=True) + itself)
    maps = spread * inverse
    itself = itself * inverse
    gain = gain_ref[...]
    lines = []
    for s in range(seqs):
        one, two = s * rows, s * rows + pad
        weight = maps[one:two] - lam * maps[two : two + pad]
        fresh_weight = itself[one:two] - lam * itself[two : two + pad]
        weight = jnp.concatenate((weight, jnp.zeros_like(weight)), 0).astype(jnp.bfloat16)
        out = jnp.dot(weight, values_ref[s], preferred_element_type=f32)[:pad]
        new_value = total[s : s + 1, at + width : at + 2 * width]
        out = out + fresh_weight.astype(jnp.bfloat16).astype(f32) * new_value
        out = out * lax.rsqrt(jnp.mean(out * out, 1, keepdims=True) + EPS) * gain
        lines.append(jnp.concatenate([out[h : h + 1] for h in range(heads)], 1))
    attended = jnp.concatenate(lines, 0).astype(jnp.bfloat16)
    for d in range(out_ref.shape[0]):
        out_ref[d] = attended


def run_attend(parts, lengths, keys, values, mix_lambda, head_gain):
    deep, seqs, _ = parts.shape
    vm = pl.BlockSpec(memory_space=pltpu.VMEM)
    sm = pl.BlockSpec(memory_space=pltpu.SMEM)
    cols = mix_lambda.shape[0] * head_gain.shape[0]
    return pl.pallas_call(
        attend_kernel,
        out_shape=jax.ShapeDtypeStruct((deep, seqs, cols), jnp.bfloat16),
        in_specs=[sm, sm, vm, vm, vm, vm],
        out_specs=vm,
        name="attend",
    )(lengths, mix_lambda, parts, keys, values, head_gain.reshape(1, -1))


def shards(
    tokens,
    lengths,
    cache_keys,
    cache_values,
    norm0_gain,
    query_weight,
    key_weight,
    value_weight,
    mix_lambda,
    head_gain,
    out_weight,
    norm1_gain,
    group_ids,
    member_ids,
    group_weight,
    member_weights,
    expert_gate,
    expert_up,
    expert_down,
    norm2_gain,
):
    return layer(
        tokens,
        lengths,
        cache_keys,
        cache_values,
        norm0_gain,
        jnp.concatenate((query_weight, key_weight, value_weight), 1),
        mix_lambda,
        head_gain,
        out_weight,
        norm1_gain,
        group_ids,
        member_ids,
        group_weight,
        member_weights,
        expert_gate,
        expert_up,
        expert_down,
        norm2_gain,
    )


def layer(
    tokens,
    lengths,
    cache_keys,
    cache_values,
    norm0_gain,
    proj_weight,
    mix_lambda,
    head_gain,
    out_weight,
    norm1_gain,
    group_ids,
    member_ids,
    group_weight,
    member_weights,
    expert_gate,
    expert_up,
    expert_down,
    norm2_gain,
):
    seqs, width = tokens.shape
    deep = lax.axis_size("z")
    experts = lax.axis_size(EP)
    halves = lax.axis_size("tp")
    side = lax.axis_index("tp")
    half = width // halves
    block = width // deep
    part = block // halves
    proj_cols = proj_weight.shape[1]
    expert_ids = group_ids[:, None] * EPG + member_ids
    share = group_weight[:, None] * member_weights

    weights = to_all(jnp.concatenate((proj_weight, out_weight.T), 1), ROW).reshape(block, -1)
    weight_in, weight_out = weights[:, :proj_cols], weights[:, proj_cols:]

    normed = layer_norm(tokens.astype(jnp.float32), norm0_gain).astype(jnp.bfloat16)
    named = jnp.pad(expert_ids.astype(jnp.bfloat16), ((0, 0), (0, 128 - expert_ids.shape[1])))
    leaving = jnp.concatenate(
        (
            normed.reshape(seqs, deep, block).transpose(1, 0, 2),
            jnp.broadcast_to(named[None], (deep, seqs, 128)),
        ),
        2,
    )
    arrived = swap(leaving, "z")
    columns = arrived[:, :, :block]
    targets = lax.iota(jnp.int32, experts)
    line_ids = arrived[:, :, block : block + expert_ids.shape[1]].astype(jnp.int32)
    select = jnp.any(line_ids[None] == targets[:, None, None, None], 3).astype(jnp.float32)
    partial = jnp.dot(
        columns.reshape(deep * seqs, block), weight_in, preferred_element_type=jnp.float32
    )
    received = swap(partial.reshape(deep, seqs, proj_cols), "z")
    attended = run_attend(received, lengths, cache_keys, cache_values, mix_lambda, head_gain)
    everyone = swap(attended, "z").reshape(deep * seqs, -1)
    partial_mix = lax.dot_general(
        everyone, weight_out, (((1,), (1,)), ((), ())), preferred_element_type=jnp.float32
    )
    mix = jnp.sum(lax.all_gather(partial_mix, "tp"), 0).astype(jnp.bfloat16)
    mix = mix.reshape(deep, seqs, block)
    stream = (ALPHA * columns.astype(jnp.float32) + mix.astype(jnp.float32)).astype(jnp.bfloat16)
    mine = lax.dynamic_slice_in_dim(stream, side * part, part, 2).astype(jnp.float32)
    sending = jnp.sum(select[:, :, :, None] * mine[None], 2).astype(jnp.bfloat16)
    slots = swap(sending, EP)
    own_stream = swap(stream, "z")
    own_stream = own_stream.transpose(1, 0, 2).reshape(seqs, width)
    settled_own = layer_norm(own_stream.astype(jnp.float32), norm1_gain).astype(jnp.bfloat16)

    rows = lax.all_gather(slots, "tp")
    kept, given = run_experts(side, rows, norm1_gain, expert_gate[0], expert_up[0], expert_down[0])
    taken = lax.ppermute(given, "tp", ((0, 1), (1, 0)))
    leaving = (kept + taken.astype(jnp.float32)).astype(jnp.bfloat16)
    returned = swap(leaving, EP)
    combine = jnp.sum(
        jnp.where(expert_ids[:, :, None] == targets[None, None, :], share[:, :, None], 0.0), 1
    )
    routed = jnp.sum(combine[:, :, None, None] * returned.astype(jnp.float32)[None], 1)
    routed = routed.reshape(seqs, half)
    own = lax.dynamic_slice_in_dim(settled_own, side * half, half, 1)
    mixed = ALPHA * own.astype(jnp.float32) + routed
    sums = lax.psum(jnp.stack((jnp.sum(mixed, 1), jnp.sum(mixed * mixed, 1))), "tp")
    mean = sums[0] / width
    spread = sums[1] / width - mean * mean
    result = (mixed - mean[:, None]) * lax.rsqrt(spread[:, None] + EPS) * norm2_gain
    return result.astype(jnp.bfloat16)


def solution(mesh):
    torus = Mesh(mesh.devices.reshape(8, 4, 4, mesh.shape["tp"]), ("z", "y", "x", "tp"))
    return jax.shard_map(
        shards,
        mesh=torus,
        in_specs=(
            P(EP, None),
            P(EP),
            P(EP, None, "tp"),
            P(EP, None, "tp"),
            P(),
            P(EP, "tp"),
            P(EP, "tp"),
            P(EP, "tp"),
            P("tp"),
            P(),
            P("tp", EP),
            P(),
            P(EP),
            P(EP, None),
            P(EP),
            P(EP, None),
            P(EP, None, "tp"),
            P(EP, None, "tp"),
            P(EP, "tp", None),
            P("tp"),
        ),
        out_specs=P(EP, "tp"),
        check_vma=False,
    )
```

```python
import jax
import jax.numpy as jnp
from jax import lax
from jax.experimental import pallas as pl
from jax.experimental.pallas import tpu as pltpu
from jax.sharding import Mesh
from jax.sharding import PartitionSpec as P


EPG = 4
EP = ("z", "y", "x")
ROW = ("y", "x")

ALPHA = 2.0**0.25
EPS = 1e-05


def swap(array, axis):
    return lax.all_to_all(array, axis, 0, 0, tiled=True)


def to_all(array, axis):
    return swap(jnp.broadcast_to(array[None], (lax.axis_size(axis), *array.shape)), axis)


def around(array, axis):
    size = lax.axis_size(axis)
    return [array] + [
        lax.ppermute(array, axis, [(i, (i + j) % size) for i in range(size)])
        for j in range(1, size)
    ]


def layer_norm(values, gain):
    mean = jnp.mean(values, -1, keepdims=True)
    spread = jnp.mean(jnp.square(values - mean), -1, keepdims=True)
    return (values - mean) * lax.rsqrt(spread + EPS) * gain


def fast(array):
    return pltpu.with_memory_space_constraint(array, pltpu.VMEM)


VM = pl.BlockSpec(memory_space=pltpu.VMEM)
SM = pl.BlockSpec(memory_space=pltpu.SMEM)
SMALL = pltpu.CompilerParams(vmem_limit_bytes=16 * 2**20)


def order_kernel(place_ref, *refs):
    out_ref = refs[-1]
    tall, wide = len(refs) - 1, refs[0].shape[0] // 16
    for dy in range(tall):
        for dx in range(wide):
            y = lax.rem(place_ref[0] + tall - dy, tall)
            x = lax.rem(place_ref[1] + wide - dx, wide)
            at = pl.multiple_of((y * wide + x) * 16, 16)
            out_ref[pl.ds(at, 16)] = refs[dy][dx * 16 : (dx + 1) * 16]


def order(place, blocks):
    rows, cols = blocks[0].shape
    return pl.pallas_call(
        order_kernel,
        out_shape=jax.ShapeDtypeStruct((rows * len(blocks), cols), blocks[0].dtype),
        in_specs=[SM] + [VM] * len(blocks),
        out_specs=VM,
        compiler_params=SMALL,
        name="order",
    )(place, *(fast(b) for b in blocks))


def outproj_kernel(heads_ref, weight_ref, out_ref, rows_ref):
    deep, seqs, _ = heads_ref.shape
    heads = jnp.concatenate([heads_ref[d].astype(jnp.float32) for d in range(deep)], 0)
    rows_ref[...] = lax.dot_general(
        heads.astype(jnp.bfloat16),
        weight_ref[...],
        (((1,), (1,)), ((), ())),
        preferred_element_type=jnp.float32,
    )
    for i in range(seqs):
        out_ref[i] = jnp.concatenate(
            [rows_ref[d * seqs + i : d * seqs + i + 1] for d in range(deep)], 0
        )


def outproj(heads, weight):
    deep, seqs, _ = heads.shape
    block = weight.shape[0]
    return pl.pallas_call(
        outproj_kernel,
        out_shape=jax.ShapeDtypeStruct((seqs, deep, block), jnp.float32),
        in_specs=[VM, VM],
        out_specs=VM,
        scratch_shapes=[pltpu.VMEM((seqs * deep, block), jnp.float32)],
        compiler_params=SMALL,
        name="outproj",
    )(fast(heads), fast(weight))


def build_kernel(side_ref, own_ref, other_ref, columns_ref, ids_ref, out_ref, stream_ref):
    seqs, _, block = own_ref.shape
    part = block // 2
    at = pl.multiple_of(side_ref[0] * part, part)
    rows, names = [], []
    for i in range(seqs):
        mix = (own_ref[i] + other_ref[i]).astype(jnp.bfloat16).astype(jnp.float32)
        stream_ref[i] = (ALPHA * columns_ref[i] + mix).astype(jnp.bfloat16).astype(jnp.float32)
        rows.append(stream_ref[i, :, pl.ds(at, part)])
        names.append([ids_ref[i, :, k * part : (k + 1) * part] for k in range(2)])
    for e in range(out_ref.shape[0]):
        value = jnp.zeros_like(rows[0])
        for row, (one, two) in zip(rows, names, strict=True):
            value = jnp.where((one == e) | (two == e), row, value)
        out_ref[e] = value.astype(jnp.bfloat16)


def build(side, own, other, columns, ids, experts):
    seqs, deep, block = own.shape
    return pl.pallas_call(
        build_kernel,
        out_shape=(
            jax.ShapeDtypeStruct((experts, deep, block // 2), jnp.bfloat16),
            jax.ShapeDtypeStruct((seqs, deep, block), jnp.float32),
        ),
        in_specs=[SM] + [VM] * 4,
        out_specs=(VM, VM),
        compiler_params=SMALL,
        name="build",
    )(side, fast(own), fast(other), fast(columns), fast(ids))


def lay_kernel(place_ref, stream_ref, *out_refs):
    seqs, deep, _ = stream_ref.shape
    for j, out_ref in enumerate(out_refs):
        z = lax.rem(place_ref[0] + j, deep)
        rows = [stream_ref[i, pl.ds(z, 1), :] for i in range(seqs)]
        out_ref[...] = jnp.concatenate(rows, 0).astype(jnp.bfloat16)


def lay(place, stream):
    seqs, deep, block = stream.shape
    return pl.pallas_call(
        lay_kernel,
        out_shape=(jax.ShapeDtypeStruct((seqs, block), jnp.bfloat16),) * deep,
        in_specs=[SM, VM],
        out_specs=(VM,) * deep,
        compiler_params=SMALL,
        name="lay",
    )(place, stream)


def settle_kernel(place_ref, side_ref, gain_ref, *refs):
    out_ref, row_ref = refs[-2:]
    deep = len(refs) - 2
    block = refs[0].shape[1]
    for j in range(deep):
        z = lax.rem(place_ref[0] + deep - j, deep)
        at = pl.multiple_of(z * block, block)
        row_ref[:, pl.ds(at, block)] = refs[j][...].astype(jnp.float32)
    values = row_ref[...]
    mean = jnp.mean(values, 1, keepdims=True)
    off = values - mean
    scale = lax.rsqrt(jnp.mean(off * off, 1, keepdims=True) + EPS)
    settled = (off * scale * gain_ref[...]).astype(jnp.bfloat16)
    row_ref[...] = ALPHA * settled.astype(jnp.float32)
    tiles = out_ref.shape[1]
    for j in range(tiles):
        at = pl.multiple_of((side_ref[0] * tiles + j) * 128, 128)
        out_ref[:, j, :] = row_ref[:, pl.ds(at, 128)]


def settle(place, side, gain, blocks):
    seqs, block = blocks[0].shape
    width = block * len(blocks)
    return pl.pallas_call(
        settle_kernel,
        out_shape=jax.ShapeDtypeStruct((seqs, width // 256, 128), jnp.float32),
        in_specs=[SM, SM] + [VM] * (1 + len(blocks)),
        out_specs=VM,
        scratch_shapes=[pltpu.VMEM((seqs, width), jnp.float32)],
        compiler_params=SMALL,
        name="settle",
    )(place, side, gain.reshape(1, -1), *blocks)


def combine_kernel(ids_ref, share_ref, returned_ref, residual_ref, mixed_ref, stats_ref):
    seqs, topk = residual_ref.shape[0], 2
    for i in range(seqs):
        mixed = residual_ref[i]
        for k in range(topk):
            row = returned_ref[ids_ref[i * topk + k]].astype(jnp.float32)
            mixed = mixed + share_ref[i * topk + k] * row
        mixed_ref[i] = mixed
        for at, value in ((i, mixed), (seqs + i, mixed * mixed)):
            total = jnp.sum(jnp.sum(value, 0, keepdims=True), 1, keepdims=True)
            stats_ref[at : at + 1] = jnp.broadcast_to(total, (1, 128))


def run_combine(ids, share, returned, residual):
    seqs = residual.shape[0]
    return pl.pallas_call(
        combine_kernel,
        out_shape=(
            jax.ShapeDtypeStruct(residual.shape, jnp.float32),
            jax.ShapeDtypeStruct((2 * seqs, 128), jnp.float32),
        ),
        in_specs=[SM, SM, VM, VM],
        out_specs=(VM, VM),
        compiler_params=SMALL,
        name="combine",
    )(ids.reshape(-1), share.reshape(-1), fast(returned), fast(residual))


def finish_kernel(mixed_ref, own_ref, other_ref, gain_ref, out_ref):
    seqs, tiles, _ = mixed_ref.shape
    width = 2 * tiles * 128
    stats = (own_ref[...] + other_ref[...]) * (1.0 / width)
    mean, second = stats[:seqs], stats[seqs:]
    scale = lax.rsqrt(second - mean * mean + EPS)
    for j in range(tiles):
        at = slice(j * 128, (j + 1) * 128)
        value = (mixed_ref[:, j, :] - mean) * scale * gain_ref[:, at]
        out_ref[:, at] = value.astype(jnp.bfloat16)


def finish(mixed, own, other, gain):
    seqs, tiles, _ = mixed.shape
    return pl.pallas_call(
        finish_kernel,
        out_shape=jax.ShapeDtypeStruct((seqs, tiles * 128), jnp.bfloat16),
        in_specs=[VM] * 4,
        out_specs=VM,
        compiler_params=SMALL,
        name="finish",
    )(fast(mixed), fast(own), fast(other), gain.reshape(1, -1))


def hidden_kernel(
    side_ref, own_ref, other_ref, gain_ref, gate_ref, up_ref, down_ref, hidden_ref, given_ref, settled_ref
):
    sources, deep, part = own_ref.shape
    line = sources // deep
    slots = line * deep
    width = gate_ref.shape[0]
    half = width // 2
    side = side_ref[0]

    def pieces():
        for c in range(deep):
            for ref, t in ((own_ref, side), (other_ref, 1 - side)):
                block = ref[c * line : (c + 1) * line].astype(jnp.float32)
                yield block.reshape(slots, part), pl.multiple_of((2 * c + t) * part, part)

    total = jnp.zeros((slots, part), jnp.float32)
    for piece, _ in pieces():
        total = total + piece
    mean = jnp.sum(total, 1, keepdims=True) * (1.0 / width)
    square = jnp.zeros((slots, part), jnp.float32)
    for piece, _ in pieces():
        off = piece - mean
        square = square + off * off
    scale = lax.rsqrt(jnp.sum(square, 1, keepdims=True) * (1.0 / width) + EPS)
    for piece, at in pieces():
        value = (piece - mean) * scale * gain_ref[:, pl.ds(at, part)]
        settled_ref[:, pl.ds(at, part)] = value.astype(jnp.bfloat16)
    settled = settled_ref[...]
    gate = jnp.dot(settled, gate_ref[...], preferred_element_type=jnp.float32)
    upward = jnp.dot(settled, up_ref[...], preferred_element_type=jnp.float32)
    hidden = (gate * jax.nn.sigmoid(gate) * upward).astype(jnp.bfloat16)
    hidden_ref[...] = hidden
    down = down_ref[:, pl.ds(pl.multiple_of((1 - side) * half, half), half)]
    tiles = in_tiles(jnp.dot(hidden, down, preferred_element_type=jnp.float32))
    tiles = tiles.astype(jnp.bfloat16)
    for p in range(line):
        for s in range(deep):
            given_ref[s * line + p] = tiles[p * deep + s]


def in_tiles(output):
    pieces = [output[:, j * 128 : (j + 1) * 128] for j in range(output.shape[1] // 128)]
    return jnp.transpose(jnp.stack(pieces, 0), (1, 0, 2))


def down_kernel(side_ref, hidden_ref, down_ref, taken_ref, out_ref):
    half = down_ref.shape[1] // 2
    line = 16
    deep = out_ref.shape[0] // line
    down = down_ref[:, pl.ds(pl.multiple_of(side_ref[0] * half, half), half)]
    tiles = in_tiles(jnp.dot(hidden_ref[...], down, preferred_element_type=jnp.float32))
    for p in range(line):
        for s in range(deep):
            both = tiles[p * deep + s] + taken_ref[s * line + p].astype(jnp.float32)
            out_ref[s * line + p] = both.astype(jnp.bfloat16)


def run_hidden(side, own, other, gain, gate, up, down):
    sources, _, _ = own.shape
    width, ff = gate.shape
    return pl.pallas_call(
        hidden_kernel,
        out_shape=(
            pltpu.VMEM((sources, ff), jnp.bfloat16),
            pltpu.VMEM((sources, width // 256, 128), jnp.bfloat16),
        ),
        in_specs=[SM] + [VM] * 6,
        out_specs=(VM, VM),
        scratch_shapes=[pltpu.VMEM((sources, width), jnp.bfloat16)],
        compiler_params=SMALL,
        name="hidden",
    )(side, fast(own), fast(other), gain.reshape(1, -1), fast(gate), fast(up), fast(down))


def run_down(side, hidden, down, taken):
    return pl.pallas_call(
        down_kernel,
        out_shape=pltpu.VMEM(taken.shape, jnp.bfloat16),
        in_specs=[SM] + [VM] * 3,
        out_specs=VM,
        compiler_params=SMALL,
        name="down",
    )(side, fast(hidden), fast(down), fast(taken))


def attend_kernel(
    lengths_ref, lambda_ref, parts_ref, keys_ref, far_ref, gain_ref, out_ref, values_ref, arrived
):
    loading = pltpu.make_async_copy(far_ref, values_ref, arrived)
    loading.start()
    deep, seqs, _ = parts_ref.shape
    _, width = keys_ref.shape[1:]
    hwidth = width // 2
    heads = lambda_ref.shape[0]
    pad = 4
    rows = 2 * pad
    f32 = jnp.float32
    total = parts_ref[0]
    for d in range(1, deep):
        total = total + parts_ref[d]
    total = total.astype(jnp.bfloat16).astype(f32)
    first = lax.broadcasted_iota(jnp.int32, (1, width), 1) < hwidth
    blank = jnp.zeros((1, width), f32)
    at = heads * width
    scores, fresh = [], []
    for s in range(seqs):
        query = [total[s : s + 1, h * width : (h + 1) * width] for h in range(heads)]
        ones = [jnp.where(first, q, 0.0) for q in query] + [blank] * (pad - heads)
        twos = [jnp.where(first, 0.0, q) for q in query] + [blank] * (pad - heads)
        grid = jnp.concatenate(ones + twos, 0)
        new_key = total[s : s + 1, at : at + width]
        fresh.append(jnp.sum(grid * new_key, 1, keepdims=True))
        scores.append(
            lax.dot_general(
                grid.astype(jnp.bfloat16),
                keys_ref[s],
                (((1,), (1,)), ((), ())),
                preferred_element_type=f32,
            )
        )
    scale = hwidth**-0.5
    cached = jnp.concatenate(scores, 0) * scale
    newest = jnp.concatenate(fresh, 0) * scale
    row = lax.broadcasted_iota(jnp.int32, (seqs * rows, 1), 0)
    filled = jnp.zeros((seqs * rows, 1), jnp.int32)
    lam = jnp.zeros((pad, 1), f32)
    for s in range(seqs):
        filled = jnp.where(row // rows == s, lengths_ref[s], filled)
    side_row = lax.broadcasted_iota(jnp.int32, (pad, 1), 0)
    for h in range(heads):
        lam = jnp.where(side_row == h, lambda_ref[h], lam)
    valid = lax.broadcasted_iota(jnp.int32, cached.shape, 1) < filled
    highest = jnp.maximum(jnp.max(jnp.where(valid, cached, -1e30), 1, keepdims=True), newest)
    spread = jnp.where(valid, jnp.exp(cached - highest), 0.0)
    itself = jnp.exp(newest - highest)
    inverse = 1.0 / (jnp.sum(spread, 1, keepdims=True) + itself)
    maps = spread * inverse
    itself = itself * inverse
    gain = gain_ref[...]
    loading.wait()
    lines = []
    for s in range(seqs):
        one, two = s * rows, s * rows + pad
        weight = maps[one:two] - lam * maps[two : two + pad]
        fresh_weight = itself[one:two] - lam * itself[two : two + pad]
        weight = jnp.concatenate((weight, jnp.zeros_like(weight)), 0).astype(jnp.bfloat16)
        out = jnp.dot(weight, values_ref[s], preferred_element_type=f32)[:pad]
        new_value = total[s : s + 1, at + width : at + 2 * width]
        out = out + fresh_weight.astype(jnp.bfloat16).astype(f32) * new_value
        out = out * lax.rsqrt(jnp.mean(out * out, 1, keepdims=True) + EPS) * gain
        lines.append(jnp.concatenate([out[h : h + 1] for h in range(heads)], 1))
    attended = jnp.concatenate(lines, 0).astype(jnp.bfloat16)
    for d in range(out_ref.shape[0]):
        out_ref[d] = attended


def run_attend(parts, lengths, keys, values, mix_lambda, head_gain):
    deep, seqs, _ = parts.shape
    cols = mix_lambda.shape[0] * head_gain.shape[0]
    return pl.pallas_call(
        attend_kernel,
        out_shape=pltpu.VMEM((deep, seqs, cols), jnp.bfloat16),
        in_specs=[SM, SM, VM, VM, pl.BlockSpec(memory_space=pl.ANY), VM],
        out_specs=VM,
        scratch_shapes=[pltpu.VMEM(values.shape, values.dtype), pltpu.SemaphoreType.DMA],
        compiler_params=SMALL,
        name="attend",
    )(lengths, mix_lambda, fast(parts), fast(keys), values, head_gain.reshape(1, -1))


def shards(
    tokens,
    lengths,
    cache_keys,
    cache_values,
    norm0_gain,
    query_weight,
    key_weight,
    value_weight,
    mix_lambda,
    head_gain,
    out_weight,
    norm1_gain,
    group_ids,
    member_ids,
    group_weight,
    member_weights,
    expert_gate,
    expert_up,
    expert_down,
    norm2_gain,
):
    return layer(
        tokens,
        lengths,
        cache_keys,
        cache_values,
        norm0_gain,
        (query_weight, key_weight, value_weight),
        mix_lambda,
        head_gain,
        out_weight,
        norm1_gain,
        group_ids,
        member_ids,
        group_weight,
        member_weights,
        expert_gate,
        expert_up,
        expert_down,
        norm2_gain,
    )


def layer(
    tokens,
    lengths,
    cache_keys,
    cache_values,
    norm0_gain,
    proj_weights,
    mix_lambda,
    head_gain,
    out_weight,
    norm1_gain,
    group_ids,
    member_ids,
    group_weight,
    member_weights,
    expert_gate,
    expert_up,
    expert_down,
    norm2_gain,
):
    seqs, width = tokens.shape
    deep = lax.axis_size("z")
    experts = lax.axis_size(EP)
    halves = lax.axis_size("tp")
    side = lax.axis_index("tp")
    block = width // deep
    part = block // halves
    proj_cols = sum(w.shape[1] for w in proj_weights)
    expert_ids = group_ids[:, None] * EPG + member_ids
    share = group_weight[:, None] * member_weights

    weight_in = to_all(jnp.concatenate(proj_weights, 1), ROW).reshape(block, proj_cols)
    line_out = jnp.concatenate(around(out_weight.T, "x"), 0)
    blocks = around(line_out, "y")
    place = jnp.stack((lax.axis_index("y"), lax.axis_index("x")))
    weight_out = order(place, blocks)

    normed = layer_norm(tokens.astype(jnp.float32), norm0_gain).astype(jnp.bfloat16)
    named = jnp.repeat(expert_ids.astype(jnp.bfloat16), part, axis=1)
    leaving = jnp.concatenate(
        (
            normed.reshape(seqs, deep, block).transpose(1, 0, 2),
            jnp.broadcast_to(named[None], (deep, *named.shape)),
        ),
        2,
    )
    arrived = swap(leaving, "z")
    columns = arrived[:, :, :block].reshape(deep * seqs, block)
    partial = jnp.dot(columns, weight_in, preferred_element_type=jnp.float32)
    received = swap(partial.reshape(deep, seqs, proj_cols), "z")
    line = arrived.astype(jnp.float32).transpose(1, 0, 2)
    line_columns, line_ids = line[:, :, :block], line[:, :, block:]
    attended = run_attend(received, lengths, cache_keys, cache_values, mix_lambda, head_gain)
    everyone = swap(attended, "z")
    core = side.reshape(1)
    depth = lax.axis_index("z").reshape(1)
    partial_mix = outproj(everyone, weight_out)
    other_mix = lax.ppermute(partial_mix, "tp", ((0, 1), (1, 0)))
    sending, stream = build(core, partial_mix, other_mix, line_columns, line_ids, experts)
    slots = swap(sending, EP)
    laid = lay(depth, stream)
    pieces = [laid[0]]
    for j in range(1, deep):
        pairs = [(z, (z + j) % deep) for z in range(deep)]
        pieces.append(lax.ppermute(laid[j], "z", pairs))
    residual = settle(depth, core, norm1_gain, pieces)

    slots_other = lax.ppermute(slots, "tp", ((0, 1), (1, 0)))
    down = expert_down[0]
    hidden, given = run_hidden(
        core, slots, slots_other, norm1_gain, expert_gate[0], expert_up[0], down
    )
    taken = lax.ppermute(given, "tp", ((0, 1), (1, 0)))
    leaving = run_down(core, hidden, down, taken)
    returned = swap(leaving, EP)
    mixed, stats = run_combine(expert_ids, share, returned, residual)
    other_stats = lax.ppermute(stats, "tp", ((0, 1), (1, 0)))
    return finish(mixed, stats, other_stats, norm2_gain)


def solution(mesh):
    torus = Mesh(mesh.devices.reshape(8, 4, 4, mesh.shape["tp"]), ("z", "y", "x", "tp"))
    return jax.shard_map(
        shards,
        mesh=torus,
        in_specs=(
            P(EP, None),
            P(EP),
            P(EP, None, "tp"),
            P(EP, None, "tp"),
            P(),
            P(EP, "tp"),
            P(EP, "tp"),
            P(EP, "tp"),
            P("tp"),
            P(),
            P("tp", EP),
            P(),
            P(EP),
            P(EP, None),
            P(EP),
            P(EP, None),
            P(EP, None, "tp"),
            P(EP, None, "tp"),
            P(EP, "tp", None),
            P("tp"),
        ),
        out_specs=P(EP, "tp"),
        check_vma=False,
    )
```

```python
import jax
import jax.numpy as jnp
from jax import lax
from jax.experimental import pallas as pl
from jax.experimental.pallas import tpu as pltpu
from jax.sharding import Mesh
from jax.sharding import PartitionSpec as P


EPG = 4
EP = ("z", "y", "x")
ROW = ("y", "x")

ALPHA = 2.0**0.25
EPS = 1e-05


def swap(array, axis):
    return lax.all_to_all(array, axis, 0, 0, tiled=True)


def to_all(array, axis):
    return swap(jnp.broadcast_to(array[None], (lax.axis_size(axis), *array.shape)), axis)


def trade(array):
    return lax.ppermute(array, "tp", ((0, 1), (1, 0)))


def send(blocks):
    deep = lax.axis_size("z")
    moved = []
    for j in range(1, len(blocks)):
        pairs = [
            (2 * z + t, 2 * ((z + (1 - 2 * t) * j) % deep) + t)
            for z in range(deep)
            for t in range(2)
        ]
        moved.append(lax.ppermute(blocks[j], ("z", "tp"), pairs))
    return moved


def fast(array):
    return pltpu.with_memory_space_constraint(array, pltpu.VMEM)


VM = pl.BlockSpec(memory_space=pltpu.VMEM)
SM = pl.BlockSpec(memory_space=pltpu.SMEM)
FAR = pl.BlockSpec(memory_space=pltpu.HBM)
SMALL = pltpu.CompilerParams(vmem_limit_bytes=16 * 2**20)


def norm_kernel(place_ref, side_ref, group_ref, member_ref, tokens_ref, gain_ref, *refs):
    out_refs, row_ref = refs[:-1], refs[-1]
    deep = 2 * (len(out_refs) - 1)
    seqs, width = tokens_ref.shape
    block = width // deep
    values = tokens_ref[...].astype(jnp.float32)
    off = values - jnp.mean(values, 1, keepdims=True)
    scale = lax.rsqrt(jnp.mean(off * off, 1, keepdims=True) + EPS)
    row_ref[...] = off * scale * gain_ref[...]
    names = []
    for i in range(seqs):
        ids = [group_ref[i] * EPG + member_ref[2 * i + k] for k in range(2)]
        names.append(jnp.concatenate([jnp.full((1, block // 2), e, jnp.int32) for e in ids], 1))
    named = jnp.concatenate(names, 0).astype(jnp.float32).astype(jnp.bfloat16)
    for j, out_ref in enumerate(out_refs):
        at = pl.multiple_of(apart(place_ref, side_ref, j, deep) * block, block)
        out_ref[:, :block] = row_ref[:, pl.ds(at, block)].astype(jnp.bfloat16)
        out_ref[:, block:] = named


def norm(place, side, groups, members, tokens, gain, deep):
    seqs, width = tokens.shape
    count = deep // 2 + 1
    return pl.pallas_call(
        norm_kernel,
        out_shape=(jax.ShapeDtypeStruct((seqs, 2 * width // deep), jnp.bfloat16),) * count,
        in_specs=[SM, SM, SM, SM, VM, VM],
        out_specs=(VM,) * count,
        scratch_shapes=[pltpu.VMEM((seqs, width), jnp.float32)],
        compiler_params=SMALL,
        name="norm",
    )(place, side, groups, members.reshape(-1), tokens, gain.reshape(1, -1))


def project_kernel(place_ref, side_ref, weight_ref, *refs):
    blocks, out_ref = refs[:-1], refs[-1]
    deep = len(blocks)
    width = weight_ref.shape[0]
    seqs = blocks[0].shape[0]
    columns = jnp.concatenate([b[:, :width].astype(jnp.float32) for b in blocks], 0)
    partial = jnp.dot(
        columns.astype(jnp.bfloat16),
        weight_ref[:, : out_ref.shape[2]],
        preferred_element_type=jnp.float32,
    )
    for j in range(deep):
        out_ref[apart(place_ref, side_ref, -j, deep)] = partial[j * seqs : (j + 1) * seqs]


def project(place, side, weights, blocks, cols):
    return pl.pallas_call(
        project_kernel,
        out_shape=jax.ShapeDtypeStruct((len(blocks), blocks[0].shape[0], cols), jnp.float32),
        in_specs=[SM, SM, VM] + [VM] * len(blocks),
        out_specs=VM,
        compiler_params=SMALL,
        name="project",
    )(place, side, fast(weights), *blocks)


def line_kernel(place_ref, side_ref, *refs):
    blocks, out_ref = refs[:-1], refs[-1]
    deep = len(blocks)
    for j in range(deep):
        z = apart(place_ref, side_ref, -j, deep)
        values = blocks[j][...].astype(jnp.float32)
        for i in range(values.shape[0]):
            out_ref[i, pl.ds(z, 1), :] = values[i : i + 1]


def in_line(place, side, blocks):
    seqs, cols = blocks[0].shape
    return pl.pallas_call(
        line_kernel,
        out_shape=jax.ShapeDtypeStruct((seqs, len(blocks), cols), jnp.float32),
        in_specs=[SM, SM] + [VM] * len(blocks),
        out_specs=VM,
        compiler_params=SMALL,
        name="line",
    )(place, side, *blocks)


def outproj_kernel(heads_ref, weight_ref, out_ref, rows_ref):
    deep, seqs, cols = heads_ref.shape
    heads = jnp.concatenate([heads_ref[d].astype(jnp.float32) for d in range(deep)], 0)
    rows_ref[...] = lax.dot_general(
        heads.astype(jnp.bfloat16),
        weight_ref[:, weight_ref.shape[1] - cols :],
        (((1,), (1,)), ((), ())),
        preferred_element_type=jnp.float32,
    )
    for i in range(seqs):
        out_ref[i] = jnp.concatenate(
            [rows_ref[d * seqs + i : d * seqs + i + 1] for d in range(deep)], 0
        )


def outproj(heads, weight):
    deep, seqs, _ = heads.shape
    block = weight.shape[0]
    return pl.pallas_call(
        outproj_kernel,
        out_shape=jax.ShapeDtypeStruct((seqs, deep, block), jnp.float32),
        in_specs=[VM, VM],
        out_specs=VM,
        scratch_shapes=[pltpu.VMEM((seqs * deep, block), jnp.float32)],
        compiler_params=SMALL,
        name="outproj",
    )(fast(heads), fast(weight))


def build_kernel(side_ref, own_ref, other_ref, line_ref, out_ref, stream_ref):
    seqs, _, block = own_ref.shape
    part = block // 2
    at = pl.multiple_of(side_ref[0] * part, part)
    rows, names = [], []
    for i in range(seqs):
        mix = (own_ref[i] + other_ref[i]).astype(jnp.bfloat16).astype(jnp.float32)
        stream = ALPHA * line_ref[i, :, :block] + mix
        stream_ref[i] = stream.astype(jnp.bfloat16).astype(jnp.float32)
        rows.append(stream_ref[i, :, pl.ds(at, part)])
        names.append([line_ref[i, :, block + k * part : block + (k + 1) * part] for k in range(2)])
    for e in range(out_ref.shape[0]):
        value = jnp.zeros_like(rows[0])
        for row, (one, two) in zip(rows, names, strict=True):
            value = jnp.where((one == e) | (two == e), row, value)
        out_ref[e] = value.astype(jnp.bfloat16)


def build(side, own, other, line, experts):
    seqs, deep, block = own.shape
    return pl.pallas_call(
        build_kernel,
        out_shape=(
            jax.ShapeDtypeStruct((experts, deep, block // 2), jnp.bfloat16),
            jax.ShapeDtypeStruct((seqs, deep, block), jnp.float32),
        ),
        in_specs=[SM] + [VM] * 3,
        out_specs=(VM, VM),
        compiler_params=SMALL,
        name="build",
    )(side, fast(own), fast(other), fast(line))


def apart(place_ref, side_ref, steps, deep):
    return lax.rem(place_ref[0] + deep + (1 - 2 * side_ref[0]) * steps, deep)


def lay_kernel(place_ref, side_ref, stream_ref, *out_refs):
    seqs, deep, _ = stream_ref.shape
    for j, out_ref in enumerate(out_refs):
        z = apart(place_ref, side_ref, j, deep)
        rows = [stream_ref[i, pl.ds(z, 1), :] for i in range(seqs)]
        out_ref[...] = jnp.concatenate(rows, 0).astype(jnp.bfloat16)


def lay(place, side, stream):
    seqs, deep, block = stream.shape
    count = deep // 2 + 1
    return pl.pallas_call(
        lay_kernel,
        out_shape=(jax.ShapeDtypeStruct((seqs, block), jnp.bfloat16),) * count,
        in_specs=[SM, SM, VM],
        out_specs=(VM,) * count,
        compiler_params=SMALL,
        name="lay",
    )(place, side, stream)


def settle_kernel(place_ref, side_ref, gain_ref, *refs):
    out_ref, row_ref = refs[-2:]
    deep = len(refs) - 2
    block = refs[0].shape[1]
    for j in range(deep):
        at = pl.multiple_of(apart(place_ref, side_ref, -j, deep) * block, block)
        row_ref[:, pl.ds(at, block)] = refs[j][...].astype(jnp.float32)
    values = row_ref[...]
    mean = jnp.mean(values, 1, keepdims=True)
    off = values - mean
    scale = lax.rsqrt(jnp.mean(off * off, 1, keepdims=True) + EPS)
    settled = (off * scale * gain_ref[...]).astype(jnp.bfloat16)
    row_ref[...] = ALPHA * settled.astype(jnp.float32)
    tiles = out_ref.shape[1]
    for j in range(tiles):
        at = pl.multiple_of((side_ref[0] * tiles + j) * 128, 128)
        out_ref[:, j, :] = row_ref[:, pl.ds(at, 128)]


def settle(place, side, gain, blocks):
    seqs, block = blocks[0].shape
    width = block * len(blocks)
    return pl.pallas_call(
        settle_kernel,
        out_shape=jax.ShapeDtypeStruct((seqs, width // 256, 128), jnp.float32),
        in_specs=[SM, SM] + [VM] * (1 + len(blocks)),
        out_specs=VM,
        scratch_shapes=[pltpu.VMEM((seqs, width), jnp.float32)],
        compiler_params=SMALL,
        name="settle",
    )(place, side, gain.reshape(1, -1), *blocks)


def combine_kernel(ids_ref, share_ref, returned_ref, residual_ref, mixed_ref, stats_ref):
    seqs, topk = residual_ref.shape[0], 2
    for i in range(seqs):
        mixed = residual_ref[i]
        for k in range(topk):
            row = returned_ref[ids_ref[i * topk + k]].astype(jnp.float32)
            mixed = mixed + share_ref[i * topk + k] * row
        mixed_ref[i] = mixed
        for at, value in ((i, mixed), (seqs + i, mixed * mixed)):
            total = jnp.sum(jnp.sum(value, 0, keepdims=True), 1, keepdims=True)
            stats_ref[at : at + 1] = jnp.broadcast_to(total, (1, 128))


def run_combine(ids, share, returned, residual):
    seqs = residual.shape[0]
    return pl.pallas_call(
        combine_kernel,
        out_shape=(
            jax.ShapeDtypeStruct(residual.shape, jnp.float32),
            jax.ShapeDtypeStruct((2 * seqs, 128), jnp.float32),
        ),
        in_specs=[SM, SM, VM, VM],
        out_specs=(VM, VM),
        compiler_params=SMALL,
        name="combine",
    )(ids.reshape(-1), share.reshape(-1), fast(returned), fast(residual))


def finish_kernel(mixed_ref, own_ref, other_ref, gain_ref, out_ref):
    seqs, tiles, _ = mixed_ref.shape
    width = 2 * tiles * 128
    stats = (own_ref[...] + other_ref[...]) * (1.0 / width)
    mean, second = stats[:seqs], stats[seqs:]
    scale = lax.rsqrt(second - mean * mean + EPS)
    for j in range(tiles):
        at = slice(j * 128, (j + 1) * 128)
        value = (mixed_ref[:, j, :] - mean) * scale * gain_ref[:, at]
        out_ref[:, at] = value.astype(jnp.bfloat16)


def finish(mixed, own, other, gain):
    seqs, tiles, _ = mixed.shape
    return pl.pallas_call(
        finish_kernel,
        out_shape=jax.ShapeDtypeStruct((seqs, tiles * 128), jnp.bfloat16),
        in_specs=[VM] * 4,
        out_specs=VM,
        compiler_params=SMALL,
        name="finish",
    )(fast(mixed), fast(own), fast(other), gain.reshape(1, -1))


def hidden_kernel(
    side_ref, own_ref, other_ref, gain_ref, gate_ref, up_ref, down_ref, hidden_ref, given_ref, settled_ref
):
    sources, deep, part = own_ref.shape
    line = sources // deep
    slots = line * deep
    width = gate_ref.shape[0]
    half = width // 2
    side = side_ref[0]

    def pieces():
        for c in range(deep):
            for ref, t in ((own_ref, side), (other_ref, 1 - side)):
                block = ref[c * line : (c + 1) * line].astype(jnp.float32)
                yield block.reshape(slots, part), pl.multiple_of((2 * c + t) * part, part)

    total = jnp.zeros((slots, part), jnp.float32)
    for piece, _ in pieces():
        total = total + piece
    mean = jnp.sum(total, 1, keepdims=True) * (1.0 / width)
    square = jnp.zeros((slots, part), jnp.float32)
    for piece, _ in pieces():
        off = piece - mean
        square = square + off * off
    scale = lax.rsqrt(jnp.sum(square, 1, keepdims=True) * (1.0 / width) + EPS)
    for piece, at in pieces():
        value = (piece - mean) * scale * gain_ref[:, pl.ds(at, part)]
        settled_ref[:, pl.ds(at, part)] = value.astype(jnp.bfloat16)
    settled = settled_ref[...]
    gate = jnp.dot(settled, gate_ref[...], preferred_element_type=jnp.float32)
    upward = jnp.dot(settled, up_ref[...], preferred_element_type=jnp.float32)
    hidden = (gate * jax.nn.sigmoid(gate) * upward).astype(jnp.bfloat16)
    hidden_ref[...] = hidden
    down = down_ref[:, pl.ds(pl.multiple_of((1 - side) * half, half), half)]
    tiles = in_tiles(jnp.dot(hidden, down, preferred_element_type=jnp.float32))
    tiles = tiles.astype(jnp.bfloat16)
    for p in range(line):
        for s in range(deep):
            given_ref[s * line + p] = tiles[p * deep + s]


def in_tiles(output):
    pieces = [output[:, j * 128 : (j + 1) * 128] for j in range(output.shape[1] // 128)]
    return jnp.transpose(jnp.stack(pieces, 0), (1, 0, 2))


def down_kernel(side_ref, hidden_ref, down_ref, taken_ref, out_ref):
    half = down_ref.shape[1] // 2
    line = 16
    deep = out_ref.shape[0] // line
    down = down_ref[:, pl.ds(pl.multiple_of(side_ref[0] * half, half), half)]
    tiles = in_tiles(jnp.dot(hidden_ref[...], down, preferred_element_type=jnp.float32))
    for p in range(line):
        for s in range(deep):
            both = tiles[p * deep + s] + taken_ref[s * line + p].astype(jnp.float32)
            out_ref[s * line + p] = both.astype(jnp.bfloat16)


def run_hidden(side, own, other, gain, gate, up, down):
    sources, _, _ = own.shape
    width, ff = gate.shape
    return pl.pallas_call(
        hidden_kernel,
        out_shape=(
            pltpu.VMEM((sources, ff), jnp.bfloat16),
            pltpu.VMEM((sources, width // 256, 128), jnp.bfloat16),
        ),
        in_specs=[SM] + [VM] * 6,
        out_specs=(VM, VM),
        scratch_shapes=[pltpu.VMEM((sources, width), jnp.bfloat16)],
        compiler_params=SMALL,
        name="hidden",
    )(side, fast(own), fast(other), gain.reshape(1, -1), fast(gate), fast(up), fast(down))


def run_down(side, hidden, down, taken):
    return pl.pallas_call(
        down_kernel,
        out_shape=pltpu.VMEM(taken.shape, jnp.bfloat16),
        in_specs=[SM] + [VM] * 3,
        out_specs=VM,
        compiler_params=SMALL,
        name="down",
    )(side, fast(hidden), fast(down), fast(taken))


def attend_kernel(
    lengths_ref,
    lambda_ref,
    parts_ref,
    far_keys_ref,
    far_values_ref,
    gain_ref,
    out_ref,
    keys_ref,
    values_ref,
    done,
):
    loads = []
    for k, (far, near) in enumerate(((far_keys_ref, keys_ref), (far_values_ref, values_ref))):
        loads.append([])
        for s in range(near.shape[0]):
            loads[k].append(pltpu.make_async_copy(far.at[s], near.at[s], done.at[k, s]))
            loads[k][s].start()
    deep, seqs, _ = parts_ref.shape
    _, width = keys_ref.shape[1:]
    hwidth = width // 2
    heads = lambda_ref.shape[0]
    pad = 4
    rows = 2 * pad
    f32 = jnp.float32
    total = parts_ref[0]
    for d in range(1, deep):
        total = total + parts_ref[d]
    total = total.astype(jnp.bfloat16).astype(f32)
    first = lax.broadcasted_iota(jnp.int32, (1, width), 1) < hwidth
    blank = jnp.zeros((1, width), f32)
    at = heads * width
    scores, fresh = [], []
    for s in range(seqs):
        query = [total[s : s + 1, h * width : (h + 1) * width] for h in range(heads)]
        ones = [jnp.where(first, q, 0.0) for q in query] + [blank] * (pad - heads)
        twos = [jnp.where(first, 0.0, q) for q in query] + [blank] * (pad - heads)
        grid = jnp.concatenate(ones + twos, 0)
        new_key = total[s : s + 1, at : at + width]
        fresh.append(jnp.sum(grid * new_key, 1, keepdims=True))
        loads[0][s].wait()
        scores.append(
            lax.dot_general(
                grid.astype(jnp.bfloat16),
                keys_ref[s],
                (((1,), (1,)), ((), ())),
                preferred_element_type=f32,
            )
        )
    scale = hwidth**-0.5
    cached = jnp.concatenate(scores, 0) * scale
    newest = jnp.concatenate(fresh, 0) * scale
    row = lax.broadcasted_iota(jnp.int32, (seqs * rows, 1), 0)
    filled = jnp.zeros((seqs * rows, 1), jnp.int32)
    lam = jnp.zeros((pad, 1), f32)
    for s in range(seqs):
        filled = jnp.where(row // rows == s, lengths_ref[s], filled)
    side_row = lax.broadcasted_iota(jnp.int32, (pad, 1), 0)
    for h in range(heads):
        lam = jnp.where(side_row == h, lambda_ref[h], lam)
    valid = lax.broadcasted_iota(jnp.int32, cached.shape, 1) < filled
    highest = jnp.maximum(jnp.max(jnp.where(valid, cached, -1e30), 1, keepdims=True), newest)
    spread = jnp.where(valid, jnp.exp(cached - highest), 0.0)
    itself = jnp.exp(newest - highest)
    inverse = 1.0 / (jnp.sum(spread, 1, keepdims=True) + itself)
    maps = spread * inverse
    itself = itself * inverse
    gain = gain_ref[...]
    lines = []
    for s in range(seqs):
        one, two = s * rows, s * rows + pad
        weight = maps[one:two] - lam * maps[two : two + pad]
        fresh_weight = itself[one:two] - lam * itself[two : two + pad]
        weight = jnp.concatenate((weight, jnp.zeros_like(weight)), 0).astype(jnp.bfloat16)
        loads[1][s].wait()
        out = jnp.dot(weight, values_ref[s], preferred_element_type=f32)[:pad]
        new_value = total[s : s + 1, at + width : at + 2 * width]
        out = out + fresh_weight.astype(jnp.bfloat16).astype(f32) * new_value
        out = out * lax.rsqrt(jnp.mean(out * out, 1, keepdims=True) + EPS) * gain
        lines.append(jnp.concatenate([out[h : h + 1] for h in range(heads)], 1))
    attended = jnp.concatenate(lines, 0).astype(jnp.bfloat16)
    for d in range(out_ref.shape[0]):
        out_ref[d] = attended


def run_attend(parts, lengths, keys, values, mix_lambda, head_gain):
    deep, seqs, _ = parts.shape
    cols = mix_lambda.shape[0] * head_gain.shape[0]
    return pl.pallas_call(
        attend_kernel,
        out_shape=pltpu.VMEM((deep, seqs, cols), jnp.bfloat16),
        in_specs=[SM, SM, VM, FAR, FAR, VM],
        out_specs=VM,
        scratch_shapes=[
            pltpu.VMEM(keys.shape, keys.dtype),
            pltpu.VMEM(values.shape, values.dtype),
            pltpu.SemaphoreType.DMA((2, seqs)),
        ],
        compiler_params=SMALL,
        name="attend",
    )(lengths, mix_lambda, fast(parts), keys, values, head_gain.reshape(1, -1))


def shards(
    tokens,
    lengths,
    cache_keys,
    cache_values,
    norm0_gain,
    query_weight,
    key_weight,
    value_weight,
    mix_lambda,
    head_gain,
    out_weight,
    norm1_gain,
    group_ids,
    member_ids,
    group_weight,
    member_weights,
    expert_gate,
    expert_up,
    expert_down,
    norm2_gain,
):
    return layer(
        tokens,
        lengths,
        cache_keys,
        cache_values,
        norm0_gain,
        (query_weight, key_weight, value_weight),
        mix_lambda,
        head_gain,
        out_weight,
        norm1_gain,
        group_ids,
        member_ids,
        group_weight,
        member_weights,
        expert_gate,
        expert_up,
        expert_down,
        norm2_gain,
    )


def layer(
    tokens,
    lengths,
    cache_keys,
    cache_values,
    norm0_gain,
    proj_weights,
    mix_lambda,
    head_gain,
    out_weight,
    norm1_gain,
    group_ids,
    member_ids,
    group_weight,
    member_weights,
    expert_gate,
    expert_up,
    expert_down,
    norm2_gain,
):
    width = tokens.shape[1]
    deep = lax.axis_size("z")
    experts = lax.axis_size(EP)
    side = lax.axis_index("tp")
    block = width // deep
    proj_cols = sum(w.shape[1] for w in proj_weights)
    expert_ids = group_ids[:, None] * EPG + member_ids
    share = group_weight[:, None] * member_weights

    own_weights = jnp.concatenate((*proj_weights, out_weight.T), 1)
    weights = to_all(own_weights, ROW).reshape(block, own_weights.shape[1])

    core = side.reshape(1)
    depth = lax.axis_index("z").reshape(1)
    leaving = norm(depth, core, group_ids, member_ids, tokens, norm0_gain, deep)
    moved = send(leaving)
    traded = [trade(m) for m in moved[:-1]]
    arrived = [leaving[0], *moved, *traded[::-1]]
    partial = project(depth, core, weights, arrived, proj_cols)
    received = swap(partial, "z")
    attended = run_attend(
        received, lengths, cache_keys, cache_values, mix_lambda, head_gain
    )
    everyone = swap(attended, "z")
    partial_mix = outproj(everyone, weights)
    other_mix = trade(partial_mix)
    line = in_line(depth, core, arrived)
    sending, stream = build(core, partial_mix, other_mix, line, experts)
    slots = swap(sending, EP)
    laid = lay(depth, core, stream)
    moved = send(laid)
    traded = [trade(m) for m in moved[:-1]]
    residual = settle(depth, core, norm1_gain, [laid[0], *moved, *traded[::-1]])
    slots_other = trade(slots)
    down = expert_down[0]
    hidden, given = run_hidden(
        core, slots, slots_other, norm1_gain, expert_gate[0], expert_up[0], down
    )
    taken = trade(given)
    leaving = run_down(core, hidden, down, taken)
    returned = swap(leaving, EP)
    mixed, stats = run_combine(expert_ids, share, returned, residual)
    other_stats = trade(stats)
    return finish(mixed, stats, other_stats, norm2_gain)


def solution(mesh):
    torus = Mesh(mesh.devices.reshape(8, 4, 4, mesh.shape["tp"]), ("z", "y", "x", "tp"))
    return jax.shard_map(
        shards,
        mesh=torus,
        in_specs=(
            P(EP, None),
            P(EP),
            P(EP, None, "tp"),
            P(EP, None, "tp"),
            P(),
            P(EP, "tp"),
            P(EP, "tp"),
            P(EP, "tp"),
            P("tp"),
            P(),
            P("tp", EP),
            P(),
            P(EP),
            P(EP, None),
            P(EP),
            P(EP, None),
            P(EP, None, "tp"),
            P(EP, None, "tp"),
            P(EP, "tp", None),
            P("tp"),
        ),
        out_specs=P(EP, "tp"),
        check_vma=False,
    )
```

```python
import jax
import jax.numpy as jnp
from jax import lax
from jax.experimental import pallas as pl
from jax.experimental.pallas import tpu as pltpu
from jax.sharding import Mesh
from jax.sharding import PartitionSpec as P


EPG = 4
EP = ("z", "y", "x")
ROW = ("y", "x")

ALPHA = 2.0**0.25
EPS = 1e-05


def swap(array, axis):
    return lax.all_to_all(array, axis, 0, 0, tiled=True)


def to_all(array, axis):
    return swap(jnp.broadcast_to(array[None], (lax.axis_size(axis), *array.shape)), axis)


def trade(array):
    return lax.ppermute(array, "tp", ((0, 1), (1, 0)))


def send(blocks):
    deep = lax.axis_size("z")
    moved = []
    for j in range(1, len(blocks)):
        pairs = [
            (2 * z + t, 2 * ((z + (1 - 2 * t) * j) % deep) + t)
            for z in range(deep)
            for t in range(2)
        ]
        moved.append(lax.ppermute(blocks[j], ("z", "tp"), pairs))
    return moved


def fast(array):
    return pltpu.with_memory_space_constraint(array, pltpu.VMEM)


def far(array):
    return pltpu.with_memory_space_constraint(array, pltpu.HBM)


VM = pl.BlockSpec(memory_space=pltpu.VMEM)
SM = pl.BlockSpec(memory_space=pltpu.SMEM)
FAR = pl.BlockSpec(memory_space=pltpu.HBM)
SMALL = pltpu.CompilerParams(vmem_limit_bytes=16 * 2**20)


def norm_kernel(place_ref, side_ref, group_ref, member_ref, tokens_ref, gain_ref, *refs):
    out_refs, row_ref = refs[:-1], refs[-1]
    deep = 2 * (len(out_refs) - 1)
    seqs, width = tokens_ref.shape
    block = width // deep
    values = tokens_ref[...].astype(jnp.float32)
    off = values - jnp.mean(values, 1, keepdims=True)
    scale = lax.rsqrt(jnp.mean(off * off, 1, keepdims=True) + EPS)
    row_ref[...] = off * scale * gain_ref[...]
    names = []
    for i in range(seqs):
        ids = [group_ref[i] * EPG + member_ref[2 * i + k] for k in range(2)]
        names.append(jnp.concatenate([jnp.full((1, block // 2), e, jnp.int32) for e in ids], 1))
    named = jnp.concatenate(names, 0).astype(jnp.float32).astype(jnp.bfloat16)
    for j, out_ref in enumerate(out_refs):
        at = pl.multiple_of(apart(place_ref, side_ref, j, deep) * block, block)
        out_ref[:, :block] = row_ref[:, pl.ds(at, block)].astype(jnp.bfloat16)
        out_ref[:, block:] = named


def norm(place, side, groups, members, tokens, gain, deep):
    seqs, width = tokens.shape
    count = deep // 2 + 1
    return pl.pallas_call(
        norm_kernel,
        out_shape=(jax.ShapeDtypeStruct((seqs, 2 * width // deep), jnp.bfloat16),) * count,
        in_specs=[SM, SM, SM, SM, VM, VM],
        out_specs=(VM,) * count,
        scratch_shapes=[pltpu.VMEM((seqs, width), jnp.float32)],
        compiler_params=SMALL,
        name="norm",
    )(place, side, groups, members.reshape(-1), tokens, gain.reshape(1, -1))


def project_kernel(place_ref, side_ref, weight_ref, *refs):
    blocks, out_ref = refs[:-1], refs[-1]
    deep = len(blocks)
    width = weight_ref.shape[0]
    seqs = blocks[0].shape[0]
    columns = jnp.concatenate([b[:, :width].astype(jnp.float32) for b in blocks], 0)
    partial = jnp.dot(
        columns.astype(jnp.bfloat16),
        weight_ref[:, : out_ref.shape[2]],
        preferred_element_type=jnp.float32,
    )
    for j in range(deep):
        out_ref[apart(place_ref, side_ref, -j, deep)] = partial[j * seqs : (j + 1) * seqs]


def project(place, side, weights, blocks, cols):
    return pl.pallas_call(
        project_kernel,
        out_shape=jax.ShapeDtypeStruct((len(blocks), blocks[0].shape[0], cols), jnp.float32),
        in_specs=[SM, SM, VM] + [VM] * len(blocks),
        out_specs=VM,
        compiler_params=SMALL,
        name="project",
    )(place, side, fast(weights), *blocks)


def line_kernel(place_ref, side_ref, *refs):
    blocks, out_ref = refs[:-1], refs[-1]
    deep = len(blocks)
    for j in range(deep):
        z = apart(place_ref, side_ref, -j, deep)
        values = blocks[j][...].astype(jnp.float32)
        for i in range(values.shape[0]):
            out_ref[i, pl.ds(z, 1), :] = values[i : i + 1]


def in_line(place, side, blocks):
    seqs, cols = blocks[0].shape
    return pl.pallas_call(
        line_kernel,
        out_shape=jax.ShapeDtypeStruct((seqs, len(blocks), cols), jnp.float32),
        in_specs=[SM, SM] + [VM] * len(blocks),
        out_specs=VM,
        compiler_params=SMALL,
        name="line",
    )(place, side, *blocks)


def outproj_kernel(heads_ref, weight_ref, out_ref, rows_ref):
    deep, seqs, cols = heads_ref.shape
    heads = jnp.concatenate([heads_ref[d].astype(jnp.float32) for d in range(deep)], 0)
    rows_ref[...] = lax.dot_general(
        heads.astype(jnp.bfloat16),
        weight_ref[:, weight_ref.shape[1] - cols :],
        (((1,), (1,)), ((), ())),
        preferred_element_type=jnp.float32,
    )
    for i in range(seqs):
        out_ref[i] = jnp.concatenate(
            [rows_ref[d * seqs + i : d * seqs + i + 1] for d in range(deep)], 0
        )


def outproj(heads, weight):
    deep, seqs, _ = heads.shape
    block = weight.shape[0]
    return pl.pallas_call(
        outproj_kernel,
        out_shape=jax.ShapeDtypeStruct((seqs, deep, block), jnp.float32),
        in_specs=[VM, VM],
        out_specs=VM,
        scratch_shapes=[pltpu.VMEM((seqs * deep, block), jnp.float32)],
        compiler_params=SMALL,
        name="outproj",
    )(fast(heads), fast(weight))


def build_kernel(side_ref, own_ref, other_ref, line_ref, out_ref, stream_ref):
    seqs, _, block = own_ref.shape
    part = block // 2
    at = pl.multiple_of(side_ref[0] * part, part)
    rows, names = [], []
    for i in range(seqs):
        mix = (own_ref[i] + other_ref[i]).astype(jnp.bfloat16).astype(jnp.float32)
        stream = ALPHA * line_ref[i, :, :block] + mix
        stream_ref[i] = stream.astype(jnp.bfloat16).astype(jnp.float32)
        rows.append(stream_ref[i, :, pl.ds(at, part)])
        names.append([line_ref[i, :, block + k * part : block + (k + 1) * part] for k in range(2)])
    for e in range(out_ref.shape[0]):
        value = jnp.zeros_like(rows[0])
        for row, (one, two) in zip(rows, names, strict=True):
            value = jnp.where((one == e) | (two == e), row, value)
        out_ref[e] = value.astype(jnp.bfloat16)


def build(side, own, other, line, experts):
    seqs, deep, block = own.shape
    return pl.pallas_call(
        build_kernel,
        out_shape=(
            jax.ShapeDtypeStruct((experts, deep, block // 2), jnp.bfloat16),
            jax.ShapeDtypeStruct((seqs, deep, block), jnp.float32),
        ),
        in_specs=[SM] + [VM] * 3,
        out_specs=(VM, VM),
        compiler_params=SMALL,
        name="build",
    )(side, fast(own), fast(other), fast(line))


def apart(place_ref, side_ref, steps, deep):
    return lax.rem(place_ref[0] + deep + (1 - 2 * side_ref[0]) * steps, deep)


def lay_kernel(place_ref, side_ref, stream_ref, *out_refs):
    seqs, deep, _ = stream_ref.shape
    for j, out_ref in enumerate(out_refs):
        z = apart(place_ref, side_ref, j, deep)
        rows = [stream_ref[i, pl.ds(z, 1), :] for i in range(seqs)]
        out_ref[...] = jnp.concatenate(rows, 0).astype(jnp.bfloat16)


def lay(place, side, stream):
    seqs, deep, block = stream.shape
    count = deep // 2 + 1
    return pl.pallas_call(
        lay_kernel,
        out_shape=(jax.ShapeDtypeStruct((seqs, block), jnp.bfloat16),) * count,
        in_specs=[SM, SM, VM],
        out_specs=(VM,) * count,
        compiler_params=SMALL,
        name="lay",
    )(place, side, stream)


def settle_kernel(place_ref, side_ref, gain_ref, *refs):
    out_ref, row_ref = refs[-2:]
    deep = len(refs) - 2
    block = refs[0].shape[1]
    for j in range(deep):
        at = pl.multiple_of(apart(place_ref, side_ref, -j, deep) * block, block)
        row_ref[:, pl.ds(at, block)] = refs[j][...].astype(jnp.float32)
    values = row_ref[...]
    mean = jnp.mean(values, 1, keepdims=True)
    off = values - mean
    scale = lax.rsqrt(jnp.mean(off * off, 1, keepdims=True) + EPS)
    settled = (off * scale * gain_ref[...]).astype(jnp.bfloat16)
    row_ref[...] = ALPHA * settled.astype(jnp.float32)
    tiles = out_ref.shape[1]
    for j in range(tiles):
        at = pl.multiple_of((side_ref[0] * tiles + j) * 128, 128)
        out_ref[:, j, :] = row_ref[:, pl.ds(at, 128)]


def settle(place, side, gain, blocks):
    seqs, block = blocks[0].shape
    width = block * len(blocks)
    return pl.pallas_call(
        settle_kernel,
        out_shape=jax.ShapeDtypeStruct((seqs, width // 256, 128), jnp.float32),
        in_specs=[SM, SM] + [VM] * (1 + len(blocks)),
        out_specs=VM,
        scratch_shapes=[pltpu.VMEM((seqs, width), jnp.float32)],
        compiler_params=SMALL,
        name="settle",
    )(place, side, gain.reshape(1, -1), *blocks)


def combine_kernel(ids_ref, share_ref, returned_ref, residual_ref, mixed_ref, stats_ref):
    seqs, topk = residual_ref.shape[0], 2
    for i in range(seqs):
        mixed = residual_ref[i]
        for k in range(topk):
            row = returned_ref[ids_ref[i * topk + k]].astype(jnp.float32)
            mixed = mixed + share_ref[i * topk + k] * row
        mixed_ref[i] = mixed
        for at, value in ((i, mixed), (seqs + i, mixed * mixed)):
            total = jnp.sum(jnp.sum(value, 0, keepdims=True), 1, keepdims=True)
            stats_ref[at : at + 1] = jnp.broadcast_to(total, (1, 128))


def run_combine(ids, share, returned, residual):
    seqs = residual.shape[0]
    return pl.pallas_call(
        combine_kernel,
        out_shape=(
            jax.ShapeDtypeStruct(residual.shape, jnp.float32),
            jax.ShapeDtypeStruct((2 * seqs, 128), jnp.float32),
        ),
        in_specs=[SM, SM, VM, VM],
        out_specs=(VM, VM),
        compiler_params=SMALL,
        name="combine",
    )(ids.reshape(-1), share.reshape(-1), fast(returned), fast(residual))


def finish_kernel(mixed_ref, own_ref, other_ref, gain_ref, out_ref):
    seqs, tiles, _ = mixed_ref.shape
    width = 2 * tiles * 128
    stats = (own_ref[...] + other_ref[...]) * (1.0 / width)
    mean, second = stats[:seqs], stats[seqs:]
    scale = lax.rsqrt(second - mean * mean + EPS)
    for j in range(tiles):
        at = slice(j * 128, (j + 1) * 128)
        value = (mixed_ref[:, j, :] - mean) * scale * gain_ref[:, at]
        out_ref[:, at] = value.astype(jnp.bfloat16)


def finish(mixed, own, other, gain):
    seqs, tiles, _ = mixed.shape
    return pl.pallas_call(
        finish_kernel,
        out_shape=jax.ShapeDtypeStruct((seqs, tiles * 128), jnp.bfloat16),
        in_specs=[VM] * 4,
        out_specs=VM,
        compiler_params=SMALL,
        name="finish",
    )(fast(mixed), fast(own), fast(other), gain.reshape(1, -1))


def load_kernel(*refs):
    half = len(refs) // 2
    done = refs[-1]
    copies = []
    for k in range(half):
        copies.append(pltpu.make_async_copy(refs[k], refs[half + k], done.at[k]))
        copies[k].start()
    for copy in copies:
        copy.wait()


def load(*arrays):
    return pl.pallas_call(
        load_kernel,
        out_shape=tuple(pltpu.VMEM(a.shape, a.dtype) for a in arrays),
        in_specs=[FAR] * len(arrays),
        out_specs=(VM,) * len(arrays),
        scratch_shapes=[pltpu.SemaphoreType.DMA((len(arrays),))],
        compiler_params=SMALL,
        name="load",
    )(*(far(a) for a in arrays))


def hidden_kernel(
    side_ref, own_ref, other_ref, gain_ref, gate_ref, up_ref, down_ref, hidden_ref, given_ref, settled_ref
):
    sources, deep, part = own_ref.shape
    line = sources // deep
    slots = line * deep
    width = gate_ref.shape[0]
    half = width // 2
    side = side_ref[0]

    def pieces():
        for c in range(deep):
            for ref, t in ((own_ref, side), (other_ref, 1 - side)):
                block = ref[c * line : (c + 1) * line].astype(jnp.float32)
                yield block.reshape(slots, part), pl.multiple_of((2 * c + t) * part, part)

    total = jnp.zeros((slots, part), jnp.float32)
    for piece, _ in pieces():
        total = total + piece
    mean = jnp.sum(total, 1, keepdims=True) * (1.0 / width)
    square = jnp.zeros((slots, part), jnp.float32)
    for piece, _ in pieces():
        off = piece - mean
        square = square + off * off
    scale = lax.rsqrt(jnp.sum(square, 1, keepdims=True) * (1.0 / width) + EPS)
    for piece, at in pieces():
        value = (piece - mean) * scale * gain_ref[:, pl.ds(at, part)]
        settled_ref[:, pl.ds(at, part)] = value.astype(jnp.bfloat16)
    settled = settled_ref[...]
    gate = jnp.dot(settled, gate_ref[...], preferred_element_type=jnp.float32)
    upward = jnp.dot(settled, up_ref[...], preferred_element_type=jnp.float32)
    hidden = (gate * jax.nn.sigmoid(gate) * upward).astype(jnp.bfloat16)
    hidden_ref[...] = hidden
    down = down_ref[:, pl.ds(pl.multiple_of((1 - side) * half, half), half)]
    tiles = in_tiles(jnp.dot(hidden, down, preferred_element_type=jnp.float32))
    tiles = tiles.astype(jnp.bfloat16)
    for p in range(line):
        for s in range(deep):
            given_ref[s * line + p] = tiles[p * deep + s]


def in_tiles(output):
    pieces = [output[:, j * 128 : (j + 1) * 128] for j in range(output.shape[1] // 128)]
    return jnp.transpose(jnp.stack(pieces, 0), (1, 0, 2))


def down_kernel(side_ref, hidden_ref, down_ref, taken_ref, out_ref):
    half = down_ref.shape[1] // 2
    line = 16
    deep = out_ref.shape[0] // line
    down = down_ref[:, pl.ds(pl.multiple_of(side_ref[0] * half, half), half)]
    tiles = in_tiles(jnp.dot(hidden_ref[...], down, preferred_element_type=jnp.float32))
    for p in range(line):
        for s in range(deep):
            both = tiles[p * deep + s] + taken_ref[s * line + p].astype(jnp.float32)
            out_ref[s * line + p] = both.astype(jnp.bfloat16)


def run_hidden(side, own, other, gain, gate, up, down):
    sources, _, _ = own.shape
    width, ff = gate.shape
    return pl.pallas_call(
        hidden_kernel,
        out_shape=(
            pltpu.VMEM((sources, ff), jnp.bfloat16),
            pltpu.VMEM((sources, width // 256, 128), jnp.bfloat16),
        ),
        in_specs=[SM] + [VM] * 6,
        out_specs=(VM, VM),
        scratch_shapes=[pltpu.VMEM((sources, width), jnp.bfloat16)],
        compiler_params=SMALL,
        name="hidden",
    )(side, fast(own), fast(other), gain.reshape(1, -1), fast(gate), fast(up), fast(down))


def run_down(side, hidden, down, taken):
    return pl.pallas_call(
        down_kernel,
        out_shape=pltpu.VMEM(taken.shape, jnp.bfloat16),
        in_specs=[SM] + [VM] * 3,
        out_specs=VM,
        compiler_params=SMALL,
        name="down",
    )(side, fast(hidden), fast(down), fast(taken))


def attend_kernel(
    lengths_ref,
    lambda_ref,
    parts_ref,
    keys_ref,
    far_ref,
    gain_ref,
    out_ref,
    values_ref,
    done,
):
    loads = []
    for s in range(far_ref.shape[0]):
        loads.append(pltpu.make_async_copy(far_ref.at[s], values_ref.at[s], done.at[s]))
        loads[s].start()
    deep, seqs, _ = parts_ref.shape
    _, width = keys_ref.shape[1:]
    hwidth = width // 2
    heads = lambda_ref.shape[0]
    pad = 4
    rows = 2 * pad
    f32 = jnp.float32
    total = parts_ref[0]
    for d in range(1, deep):
        total = total + parts_ref[d]
    total = total.astype(jnp.bfloat16).astype(f32)
    first = lax.broadcasted_iota(jnp.int32, (1, width), 1) < hwidth
    blank = jnp.zeros((1, width), f32)
    at = heads * width
    scores, fresh = [], []
    for s in range(seqs):
        query = [total[s : s + 1, h * width : (h + 1) * width] for h in range(heads)]
        ones = [jnp.where(first, q, 0.0) for q in query] + [blank] * (pad - heads)
        twos = [jnp.where(first, 0.0, q) for q in query] + [blank] * (pad - heads)
        grid = jnp.concatenate(ones + twos, 0)
        new_key = total[s : s + 1, at : at + width]
        fresh.append(jnp.sum(grid * new_key, 1, keepdims=True))
        scores.append(
            lax.dot_general(
                grid.astype(jnp.bfloat16),
                keys_ref[s],
                (((1,), (1,)), ((), ())),
                preferred_element_type=f32,
            )
        )
    scale = hwidth**-0.5
    cached = jnp.concatenate(scores, 0) * scale
    newest = jnp.concatenate(fresh, 0) * scale
    row = lax.broadcasted_iota(jnp.int32, (seqs * rows, 1), 0)
    filled = jnp.zeros((seqs * rows, 1), jnp.int32)
    lam = jnp.zeros((pad, 1), f32)
    for s in range(seqs):
        filled = jnp.where(row // rows == s, lengths_ref[s], filled)
    side_row = lax.broadcasted_iota(jnp.int32, (pad, 1), 0)
    for h in range(heads):
        lam = jnp.where(side_row == h, lambda_ref[h], lam)
    valid = lax.broadcasted_iota(jnp.int32, cached.shape, 1) < filled
    highest = jnp.maximum(jnp.max(jnp.where(valid, cached, -1e30), 1, keepdims=True), newest)
    spread = jnp.where(valid, jnp.exp(cached - highest), 0.0)
    itself = jnp.exp(newest - highest)
    inverse = 1.0 / (jnp.sum(spread, 1, keepdims=True) + itself)
    maps = spread * inverse
    itself = itself * inverse
    gain = gain_ref[...]
    lines = []
    for s in range(seqs):
        one, two = s * rows, s * rows + pad
        weight = maps[one:two] - lam * maps[two : two + pad]
        fresh_weight = itself[one:two] - lam * itself[two : two + pad]
        weight = jnp.concatenate((weight, jnp.zeros_like(weight)), 0).astype(jnp.bfloat16)
        loads[s].wait()
        out = jnp.dot(weight, values_ref[s], preferred_element_type=f32)[:pad]
        new_value = total[s : s + 1, at + width : at + 2 * width]
        out = out + fresh_weight.astype(jnp.bfloat16).astype(f32) * new_value
        out = out * lax.rsqrt(jnp.mean(out * out, 1, keepdims=True) + EPS) * gain
        lines.append(jnp.concatenate([out[h : h + 1] for h in range(heads)], 1))
    attended = jnp.concatenate(lines, 0).astype(jnp.bfloat16)
    for d in range(out_ref.shape[0]):
        out_ref[d] = attended


def run_attend(parts, lengths, keys, values, mix_lambda, head_gain):
    deep, seqs, _ = parts.shape
    cols = mix_lambda.shape[0] * head_gain.shape[0]
    return pl.pallas_call(
        attend_kernel,
        out_shape=pltpu.VMEM((deep, seqs, cols), jnp.bfloat16),
        in_specs=[SM, SM, VM, VM, FAR, VM],
        out_specs=VM,
        scratch_shapes=[
            pltpu.VMEM(values.shape, values.dtype),
            pltpu.SemaphoreType.DMA((seqs,)),
        ],
        compiler_params=SMALL,
        name="attend",
    )(lengths, mix_lambda, fast(parts), fast(keys), far(values), head_gain.reshape(1, -1))


def shards(
    tokens,
    lengths,
    cache_keys,
    cache_values,
    norm0_gain,
    query_weight,
    key_weight,
    value_weight,
    mix_lambda,
    head_gain,
    out_weight,
    norm1_gain,
    group_ids,
    member_ids,
    group_weight,
    member_weights,
    expert_gate,
    expert_up,
    expert_down,
    norm2_gain,
):
    return layer(
        tokens,
        lengths,
        cache_keys,
        cache_values,
        norm0_gain,
        (query_weight, key_weight, value_weight),
        mix_lambda,
        head_gain,
        out_weight,
        norm1_gain,
        group_ids,
        member_ids,
        group_weight,
        member_weights,
        expert_gate,
        expert_up,
        expert_down,
        norm2_gain,
    )


def layer(
    tokens,
    lengths,
    cache_keys,
    cache_values,
    norm0_gain,
    proj_weights,
    mix_lambda,
    head_gain,
    out_weight,
    norm1_gain,
    group_ids,
    member_ids,
    group_weight,
    member_weights,
    expert_gate,
    expert_up,
    expert_down,
    norm2_gain,
):
    width = tokens.shape[1]
    deep = lax.axis_size("z")
    experts = lax.axis_size(EP)
    side = lax.axis_index("tp")
    block = width // deep
    proj_cols = sum(w.shape[1] for w in proj_weights)
    expert_ids = group_ids[:, None] * EPG + member_ids
    share = group_weight[:, None] * member_weights

    own_weights = jnp.concatenate((*proj_weights, out_weight.T), 1)
    weights = to_all(own_weights, ROW).reshape(block, own_weights.shape[1])

    core = side.reshape(1)
    depth = lax.axis_index("z").reshape(1)
    leaving = norm(depth, core, group_ids, member_ids, tokens, norm0_gain, deep)
    moved = send(leaving)
    traded = [trade(m) for m in moved[:-1]]
    arrived = [leaving[0], *moved, *traded[::-1]]
    partial = project(depth, core, weights, arrived, proj_cols)
    received = swap(partial, "z")
    attended = run_attend(
        received, lengths, cache_keys, cache_values, mix_lambda, head_gain
    )
    everyone = swap(attended, "z")
    partial_mix = outproj(everyone, weights)
    other_mix = trade(partial_mix)
    line = in_line(depth, core, arrived)
    sending, stream = build(core, partial_mix, other_mix, line, experts)
    slots = swap(sending, EP)
    laid = lay(depth, core, stream)
    moved = send(laid)
    traded = [trade(m) for m in moved[:-1]]
    residual = settle(depth, core, norm1_gain, [laid[0], *moved, *traded[::-1]])
    slots_other = trade(slots)
    (upward,) = load(expert_up[0])
    down = expert_down[0]
    hidden, given = run_hidden(core, slots, slots_other, norm1_gain, expert_gate[0], upward, down)
    taken = trade(given)
    leaving = run_down(core, hidden, down, taken)
    returned = swap(leaving, EP)
    mixed, stats = run_combine(expert_ids, share, returned, residual)
    other_stats = trade(stats)
    return finish(mixed, stats, other_stats, norm2_gain)


def solution(mesh):
    torus = Mesh(mesh.devices.reshape(8, 4, 4, mesh.shape["tp"]), ("z", "y", "x", "tp"))
    return jax.shard_map(
        shards,
        mesh=torus,
        in_specs=(
            P(EP, None),
            P(EP),
            P(EP, None, "tp"),
            P(EP, None, "tp"),
            P(),
            P(EP, "tp"),
            P(EP, "tp"),
            P(EP, "tp"),
            P("tp"),
            P(),
            P("tp", EP),
            P(),
            P(EP),
            P(EP, None),
            P(EP),
            P(EP, None),
            P(EP, None, "tp"),
            P(EP, None, "tp"),
            P(EP, "tp", None),
            P("tp"),
        ),
        out_specs=P(EP, "tp"),
        check_vma=False,
    )
```
